256 devices in a mesh: rep: 2 (over z_hi), fs: 16 (over z_lo, x), tp: 8 (over y, core).
Axes of the slice: x: 4, y: 4, z: 8 (z_hi: 2, z_lo: 4; z = z_hi * 4 + z_lo), core: 2. Of those that a mesh axis runs over, the one named last changes fastest.
Arguments:
- tokens: bfloat16 [32768, 2048], P(('rep', 'fs'), 'tp'), may hold values from -6 to 6
- mix_in_gain: bfloat16 [2048], replicated, may hold values from 0.099609375 to 1.8984375
- bgate_weight: bfloat16 [2048, 2048], P('fs', 'tp'), may hold values from -0.125 to 0.125
- cgate_weight: bfloat16 [2048, 2048], P('fs', 'tp'), may hold values from -0.125 to 0.125
- value_weight: bfloat16 [2048, 2048], P('fs', 'tp'), may hold values from -0.125 to 0.125
- conv_taps: bfloat16 [3, 2048], replicated, may hold values from -3 to 3
- out_weight: bfloat16 [2048, 2048], P('tp', 'fs'), may hold values from -0.41984465 to 0.41984465
- mix_out_gain: bfloat16 [2048], replicated, may hold values from 0.099609375 to 1.8984375
- ffn_in_gain: bfloat16 [2048], replicated, may hold values from 0.099609375 to 1.8984375
- up_weight: bfloat16 [2048, 8192], P('fs', 'tp'), may hold values from -0.125 to 0.125
- down_weight: bfloat16 [8192, 2048], P('tp', 'fs'), may hold values from -0.20992233 to 0.20992233
- ffn_out_gain: bfloat16 [2048], replicated, may hold values from 0.099609375 to 1.8984375
Outputs:
- result: bfloat16 [32768, 2048], P(('rep', 'fs'), 'tp')
The draws below stay inside these ranges and needn't reach their ends.
All inputs are finite; a program needn't handle non-finite values.
Results may differ from the reference program's by a relative error of at most 0.02.
Values may be sent and summed in bfloat16 or wider, within the bound.
A program may use at most 128 MiB of HBM per device.

```python
import jax
import jax.numpy as jnp
from jax import lax

D = 2048
CW = 2048
FF = 8192
LEN = 256
TOKENS = 32768
N_TP = 8


def rising_matrix(base, rows, cols, top):
    ramp = top ** (jnp.arange(cols, dtype=jnp.float32) / cols)
    return (base * ramp[None, :] * rows ** (-0.5)).astype(jnp.bfloat16)


def draw_out_weight(key, part):
    own_key = jax.random.fold_in(key, 11)
    base = jnp.clip(jax.random.normal(own_key, (CW, D), jnp.float32), -6.0, 6.0)
    return rising_matrix(base, CW, D, 3.0)


def draw_down_weight(key, part):
    own_key = jax.random.fold_in(key, 23)
    base = jnp.clip(jax.random.normal(own_key, (FF, D), jnp.float32), -6.0, 6.0)
    return rising_matrix(base, FF, D, 3.0)


def shard_levels(key, extent, split, least, top_value):
    def one(position, blocks):
        steps = jax.random.uniform(jax.random.fold_in(jax.random.fold_in(key, 6), position), (blocks,), jnp.float32, least / len(split), top_value / len(split))
        return jnp.repeat(jnp.exp(steps), extent[position] // blocks).reshape((-1,) + (1,) * (len(extent) - position - 1))

    level = one(*split[0])
    for cut in split[1:]:
        level = level * one(*cut)
    return level


def centred(key, extent, spread, reach, split=(), kind=jnp.bfloat16):
    level = shard_levels(key, extent, split, -0.22, 0.18) if split else 1.0
    drawn = jax.random.normal(key, extent, jnp.float32) * spread * level
    return jnp.minimum(jnp.maximum(drawn, -reach), reach).astype(kind)


def setup_inputs(seed: int = 0) -> dict:
    arg_keys = jax.random.split(jax.random.key(seed), 13)
    return {
        "tokens": centred(arg_keys[0], (TOKENS, D), 1.0, 6.0, ((0, 32), (1, 8))),
        "mix_in_gain": jnp.clip(1.0 + 0.18 * jax.random.normal(arg_keys[1], (D,), jnp.float32), 0.099609375, 1.8984375).astype(jnp.bfloat16),
        "bgate_weight": centred(arg_keys[2], (D, CW), D ** -0.5, 0.125, ((0, 16), (1, 8))),
        "cgate_weight": centred(arg_keys[3], (D, CW), D ** -0.5, 0.125, ((0, 16), (1, 8))),
        "value_weight": centred(arg_keys[4], (D, CW), D ** -0.5, 0.125, ((0, 16), (1, 8))),
        "conv_taps": centred(arg_keys[5], (3, CW), 0.6, 3.0),
        "out_weight": draw_out_weight(jax.random.fold_in(arg_keys[12], 71), 0),
        "mix_out_gain": jnp.clip(1.0 + 0.18 * jax.random.normal(arg_keys[7], (D,), jnp.float32), 0.099609375, 1.8984375).astype(jnp.bfloat16),
        "ffn_in_gain": jnp.clip(1.0 + 0.18 * jax.random.normal(arg_keys[8], (D,), jnp.float32), 0.099609375, 1.8984375).astype(jnp.bfloat16),
        "up_weight": centred(arg_keys[9], (D, FF), D ** -0.5, 0.125, ((0, 16), (1, 8))),
        "down_weight": draw_down_weight(jax.random.fold_in(arg_keys[12], 71), 0),
        "ffn_out_gain": jnp.clip(1.0 + 0.18 * jax.random.normal(arg_keys[11], (D,), jnp.float32), 0.099609375, 1.8984375).astype(jnp.bfloat16),
    }


epsilon = 1e-06

def normalize(rows, gain):
    rows = rows.astype(jnp.float32)
    factor = lax.rsqrt(lax.optimization_barrier(jnp.mean(rows * rows, axis=-1, keepdims=True)) + epsilon)
    return rows * factor * gain.astype(jnp.float32)

def block_sum(left, right, blocks):
    width = left.shape[1] // blocks

    def step(total, index):
        start = (index * width).astype(jnp.int32)
        piece_left = lax.dynamic_slice_in_dim(left, start, width, 1)
        piece_right = lax.dynamic_slice_in_dim(right, start, width, 0)
        partial_term = jnp.dot(piece_left, piece_right, preferred_element_type=jnp.float32).astype(jnp.bfloat16)
        return (total + partial_term.astype(jnp.float32), None)
    start_total = jnp.zeros((left.shape[0], right.shape[1]), jnp.float32)
    total, _ = lax.scan(step, start_total, jnp.arange(blocks, dtype=jnp.int32))
    return total

def convolve(inner, taps):
    seqs = inner.reshape(-1, LEN, inner.shape[1])
    padded = jnp.pad(seqs, ((0, 0), (1, 1), (0, 0)))
    weights = taps.astype(jnp.float32)
    out = weights[0] * padded[:, :-2] + weights[1] * padded[:, 1:-1] + weights[2] * padded[:, 2:]
    return out.reshape(inner.shape)

def reference(tokens, mix_in_gain, bgate_weight, cgate_weight, value_weight, conv_taps, out_weight, mix_out_gain, ffn_in_gain, up_weight, down_weight, ffn_out_gain):
    normed = normalize(tokens, mix_in_gain).astype(jnp.bfloat16)
    bgate = jnp.dot(normed, bgate_weight, preferred_element_type=jnp.float32).astype(jnp.bfloat16)
    cgate = jnp.dot(normed, cgate_weight, preferred_element_type=jnp.float32).astype(jnp.bfloat16)
    value = jnp.dot(normed, value_weight, preferred_element_type=jnp.float32).astype(jnp.bfloat16)
    inner = cgate.astype(jnp.float32) * value.astype(jnp.float32)
    gated = (bgate.astype(jnp.float32) * convolve(inner, conv_taps)).astype(jnp.bfloat16)
    mixed = block_sum(gated, out_weight, N_TP)
    resid = (tokens.astype(jnp.float32) + normalize(mixed, mix_out_gain)).astype(jnp.bfloat16)
    second = normalize(resid, ffn_in_gain).astype(jnp.bfloat16)
    lifted = jnp.dot(second, up_weight, preferred_element_type=jnp.float32)
    active = jnp.square(jnp.maximum(lifted, 0.0)).astype(jnp.bfloat16)
    ffn = block_sum(active, down_weight, N_TP)
    return (resid.astype(jnp.float32) + normalize(ffn, ffn_out_gain)).astype(jnp.bfloat16)
```

```python
import jax
import jax.numpy as jnp
from jax import lax
from jax.experimental import pallas as pl
from jax.experimental.pallas import tpu as pltpu
from jax.sharding import Mesh
from jax.sharding import PartitionSpec as P

EPS = 1e-6
F32 = jnp.float32
BF16 = jnp.bfloat16
LEN = 256
ROWS = 1024
W = 256
NSEQ = ROWS // LEN
NSEM = 256


class Link:
    def __init__(self, send, recv, first):
        self.send, self.recv, self.used, self.open = send, recv, first, []

    def start(self, src, dst, landed, device):
        k = self.used
        self.used += 1
        copy = pltpu.make_async_remote_copy(
            src_ref=src, dst_ref=dst, send_sem=self.send.at[k], recv_sem=self.recv.at[k],
            device_id=device, device_id_type=pl.DeviceIdType.MESH,
        )
        copy.start()
        arrival = pltpu.make_async_remote_copy(
            src_ref=landed, dst_ref=landed, send_sem=self.send.at[k], recv_sem=self.recv.at[k],
            device_id=device, device_id_type=pl.DeviceIdType.MESH,
        )
        self.open.append(copy)
        return arrival.wait_recv

    def same(self, mine, theirs, device):
        return self.start(mine, mine, theirs, device)

    def drain(self):
        for copy in self.open:
            copy.wait_send()
        self.open = []


class Here:
    def __init__(self):
        r, z, x, y, c = (lax.axis_index(n) for n in ("r", "z", "x", "y", "c"))
        self.z, self.x, self.y, self.c = z, x, y, c
        plus = lambda v, k, n: lax.rem(v + k, n)
        self.xp, self.xo, self.xm = (plus(x, k, 4) for k in (1, 2, 3))
        self.yp, self.yo, self.ym = (plus(y, k, 4) for k in (1, 2, 3))
        self.zp, self.zo, self.zm = (plus(z, k, 4) for k in (1, 2, 3))
        self.cn = 1 - c
        up, down = plus(r * 4 + z, 1, 8), plus(r * 4 + z, 7, 8)
        self.to_xp, self.to_xm = {"x": self.xp}, {"x": self.xm}
        self.to_yp, self.to_ym = {"y": self.yp}, {"y": self.ym}
        self.to_zp = {"r": up // 4, "z": lax.rem(up, 4)}
        self.to_zm = {"r": down // 4, "z": lax.rem(down, 4)}
        self.to_mate = {"c": self.cn}
        self.col = y * 2 + c


def at128(v, n=128):
    return pl.ds(pl.multiple_of(v * 128, 128), n)


class Weight:
    def __init__(self, link, here, buf, by_row):
        self.link, self.h, self.buf, self.by_row = link, here, buf, by_row
        self.half = (buf.shape[2] if by_row else buf.shape[1]) // 2

    def unit(self, z, x, part, half=None):
        if self.by_row:
            start, n = (0, 128) if half is None else (64 * half, 64)
            rows = pl.ds(pl.multiple_of(x * 128 + start, 64), n)
            return self.buf.at[z, rows, pl.ds(part * self.half, self.half)]
        q = self.half // 2
        rows = pl.ds(part * self.half, self.half) if half is None else pl.ds(part * self.half + half * q, q)
        return self.buf.at[z, rows, at128(x)]

    def line_a(self, z, half):
        if self.by_row:
            return self.buf.at[z, pl.ds(256 * half, 256), pl.ds(0, self.half)]
        q = self.half // 2
        return self.buf.at[z, pl.ds(q * half, q), :]

    def line_b(self, x, half):
        if self.by_row:
            return self.buf.at[pl.ds(2 * half, 2), at128(x), pl.ds(self.half, self.half)]
        return self.buf.at[pl.ds(2 * half, 2), pl.ds(self.half, self.half), at128(x)]

    def p1(self):
        h, u, s = self.h, self.unit, self.link.same
        a, b = u(h.z, h.x, 0), u(h.z, h.x, 1)
        self.r1 = [
            s(a, u(h.z, h.xm, 0), h.to_xp), s(a, u(h.z, h.xp, 0), h.to_xm),
            s(b, u(h.zm, h.x, 1), h.to_zp), s(b, u(h.zp, h.x, 1), h.to_zm),
        ]

    def s1(self):
        h, u, s = self.h, self.unit, self.link.same
        self.r2 = []
        for k, (wait, src, gets, dev) in enumerate((
            (self.r1[0], u(h.z, h.xm, 0, 0), u(h.z, h.xo, 0, 0), h.to_xp),
            (self.r1[1], u(h.z, h.xp, 0, 1), u(h.z, h.xo, 0, 1), h.to_xm),
            (self.r1[2], u(h.zm, h.x, 1, 0), u(h.zo, h.x, 1, 0), h.to_zp),
            (self.r1[3], u(h.zp, h.x, 1, 1), u(h.zo, h.x, 1, 1), h.to_zm),
        )):
            wait()
            self.r2.append(s(src, gets, dev))

    def s2(self):
        h, s, a, b = self.h, self.link.same, self.line_a, self.line_b
        for wait in self.r2:
            wait()
        self.rf = [
            s(a(h.z, 0), a(h.zm, 0), h.to_zp), s(a(h.z, 1), a(h.zp, 1), h.to_zm),
            s(b(h.x, 0), b(h.xm, 0), h.to_xp), s(b(h.x, 1), b(h.xp, 1), h.to_xm),
        ]
        self.rg = [
            s(a(h.z, 1), a(h.zm, 1), h.to_zp), s(a(h.z, 0), a(h.zp, 0), h.to_zm),
            s(b(h.x, 1), b(h.xm, 1), h.to_xp), s(b(h.x, 0), b(h.xp, 0), h.to_xm),
        ]

    def s3(self):
        h, s, a, b = self.h, self.link.same, self.line_a, self.line_b
        for wait, src, gets, dev in (
            (self.rf[0], a(h.zm, 0), a(h.zo, 0), h.to_zp),
            (self.rf[1], a(h.zp, 1), a(h.zo, 1), h.to_zm),
            (self.rf[2], b(h.xm, 0), b(h.xo, 0), h.to_xp),
            (self.rf[3], b(h.xp, 1), b(h.xo, 1), h.to_xm),
        ):
            wait()
            self.rg.append(s(src, gets, dev))

    def s4(self):
        for wait in self.rg:
            wait()


class Gather:
    def __init__(self, link, here, buf, row, n):
        self.link, self.h, self.buf, self.row, self.n = link, here, buf, row, n

    def piece(self, c, y, half=None):
        if half is None:
            return self.buf.at[c, y, pl.ds(self.row, self.n)]
        return self.buf.at[c, y, pl.ds(self.row + half * (self.n // 2), self.n // 2)]

    def t0(self):
        h, s, p = self.h, self.link.same, self.piece
        c, y = h.c, h.y
        self.f = [s(p(c, y, 0), p(c, h.ym, 0), h.to_yp), s(p(c, y, 1), p(c, h.yp, 1), h.to_ym)]
        self.g = [s(p(c, y, 1), p(c, h.ym, 1), h.to_yp), s(p(c, y, 0), p(c, h.yp, 0), h.to_ym)]
        self.mate = [s(p(c, y), p(h.cn, y), h.to_mate)]

    def t1(self):
        h, s, p = self.h, self.link.same, self.piece
        c = h.c
        self.f[0]()
        far = [s(p(c, h.ym, 0), p(c, h.yo, 0), h.to_yp)]
        self.f[1]()
        far.append(s(p(c, h.yp, 1), p(c, h.yo, 1), h.to_ym))
        self.far = far
        self.g[0]()
        self.mate.append(s(p(c, h.ym), p(h.cn, h.ym), h.to_mate))
        self.g[1]()
        self.mate.append(s(p(c, h.yp), p(h.cn, h.yp), h.to_mate))

    def t2(self):
        h, s, p = self.h, self.link.same, self.piece
        for wait in self.far:
            wait()
        self.mate.append(s(p(h.c, h.yo), p(h.cn, h.yo), h.to_mate))

    def t3(self):
        for wait in self.mate:
            wait()


class Reduce:
    def __init__(self, link, here, part, mate, r1, r2, seq):
        self.link, self.h, self.part, self.mate, self.r1, self.r2 = link, here, part, mate, r1, r2
        self.seq, self.row = seq, seq * LEN

    def start(self):
        h, rows = self.h, pl.ds(self.row, LEN)
        self.w0 = self.link.start(
            self.part.at[h.cn, :, rows], self.mate.at[:, rows], self.mate.at[:, rows], h.to_mate
        )

    def both(self, y, lo=0, n=LEN):
        rows = pl.ds(self.row + lo, n)
        return self.part[self.h.c, y, rows, :].astype(F32) + self.mate[y, rows, :].astype(F32)

    def b(self):
        h, half = self.h, LEN // 2
        self.w0()
        self.part[h.c, h.yo, pl.ds(self.row, LEN), :] = self.both(h.yo).astype(BF16)
        lo = self.part.at[h.c, h.yo, pl.ds(self.row, half)]
        hi = self.part.at[h.c, h.yo, pl.ds(self.row + half, half)]
        d0, d1 = self.r1.at[0, self.seq], self.r1.at[1, self.seq]
        self.w1 = [self.link.start(lo, d0, d0, h.to_yp), self.link.start(hi, d1, d1, h.to_ym)]

    def c(self):
        h, half = self.h, LEN // 2
        rows = pl.ds(self.row, LEN)
        self.w2 = []
        for k, y, dev in ((0, h.yp, h.to_yp), (1, h.ym, h.to_ym)):
            self.w1[k]()
            add = self.r1[k, self.seq].astype(F32)
            near, far = self.both(y, k * half, half) + add, self.both(y, (1 - k) * half, half)
            self.part[h.c, y, pl.ds(self.row + k * half, half), :] = near.astype(BF16)
            self.part[h.c, y, pl.ds(self.row + (1 - k) * half, half), :] = far.astype(BF16)
            dst = self.r2.at[k, rows]
            self.w2.append(self.link.start(self.part.at[h.c, y, rows], dst, dst, dev))

    def d(self):
        rows = pl.ds(self.row, LEN)
        self.w2[0]()
        self.w2[1]()
        return self.both(self.h.y) + self.r2[0, rows, :].astype(F32) + self.r2[1, rows, :].astype(F32)


def mean_factor(total):
    return lax.rsqrt(total * (1.0 / (8 * W)) + EPS)


def kernel(
    tok, bw, cw, vw, ow, uw, dw, consts, out,
    X, M, N, WB, WO, WU, WD, ACT, PA, RDA, R1A, R2A, PB, RDB, R1B, R2B, OWN, ST,
    send, recv, local,
):
    h = Here()
    link, early = Link(send, recv, 32), Link(send, recv, 0)
    own_rows = at128(h.x)
    loads = [
        pltpu.make_async_copy(tok, X.at[h.c, h.y], local.at[0]),
        pltpu.make_async_copy(bw, WB.at[h.z, own_rows, pl.ds(0, W)], local.at[1]),
        pltpu.make_async_copy(cw, WB.at[h.z, own_rows, pl.ds(W, W)], local.at[2]),
        pltpu.make_async_copy(vw, WB.at[h.z, own_rows, pl.ds(2 * W, W)], local.at[3]),
        pltpu.make_async_copy(ow, WO.at[h.z, :, own_rows], local.at[4]),
        pltpu.make_async_copy(uw, WU.at[h.z, own_rows, :], local.at[5]),
        pltpu.make_async_copy(dw, WD.at[h.z, :, own_rows], local.at[6]),
    ]
    for load in loads:
        load.start()

    peers = [
        (dy, dc, {"y": lax.rem(h.y + dy, 4), "c": lax.rem(h.c + dc, 2)})
        for dy in range(4) for dc in range(2) if dy or dc
    ]
    barrier = pltpu.get_barrier_semaphore()
    targets = [h.to_xp, h.to_xm, h.to_zp, h.to_zm] + [dev for _, _, dev in peers]
    for dev in targets:
        pl.semaphore_signal(barrier, inc=1, device_id=dev, device_id_type=pl.DeviceIdType.MESH)
    pl.semaphore_wait(barrier, len(targets))

    toks = [Gather(early, h, X, t * 512, 512) for t in range(2)]
    bcv, outw = Weight(link, h, WB, True), Weight(link, h, WO, False)
    up, down = Weight(link, h, WU, True), Weight(link, h, WD, False)
    mix = [Reduce(link, h, PA, RDA, R1A, R2A, s) for s in range(NSEQ)]
    ffn = [Reduce(link, h, PB, RDB, R1B, R2B, s) for s in range(NSEQ)]
    mids = [Gather(link, h, M, s * LEN, LEN) for s in range(NSEQ)]

    def whole(buf, rows):
        return [buf[j % 2, j // 2, rows, :].astype(F32) for j in range(8)]

    def total(pieces):
        squares = sum(p * p for p in pieces)
        return jnp.sum(squares, axis=1, keepdims=True)

    def gain(k, j):
        return consts[k : k + 1, j * W : (j + 1) * W]

    def norm_tokens(first, count):
        def tile(i, carry):
            rows = pl.ds(pl.multiple_of(first + i * 16, 16), 16)
            pieces = whole(X, rows)
            factor = mean_factor(total(pieces))
            for j in range(8):
                N[rows, j * W : (j + 1) * W] = (pieces[j] * factor * gain(0, j)).astype(BF16)
            return carry

        lax.fori_loop(0, count // 16, tile, 0)

    position = lax.broadcasted_iota(jnp.int32, (LEN, W), 0)
    own_cols = pl.ds(pl.multiple_of(h.col * W, W), W)

    def mixer(s):
        rows = pl.ds(s * LEN, LEN)
        three = jnp.dot(N[rows, :], WB[...].reshape(8 * W, 3 * W), preferred_element_type=F32)
        b, c, v = (three[:, k * W : (k + 1) * W].astype(BF16).astype(F32) for k in range(3))
        inner = c * v
        before = jnp.where(position == 0, 0.0, pltpu.roll(inner, 1, 0))
        after = jnp.where(position == LEN - 1, 0.0, pltpu.roll(inner, LEN - 1, 0))
        taps = [consts[4 + k : 5 + k, own_cols] for k in range(3)]
        conv = taps[0] * before + taps[1] * inner + taps[2] * after
        return (b * conv).astype(BF16)

    def spread(left, weight, part, s):
        rows = pl.ds(s * LEN, LEN)
        for y in range(4):
            piece = jnp.dot(left, weight[y], preferred_element_type=F32).astype(BF16)
            part[0, y, rows, :] = piece[:, :W]
            part[1, y, rows, :] = piece[:, W:]

    def A(s, before_out=None):
        gated = mixer(s)
        if before_out:
            before_out()
        spread(gated, WO, PA, s)
        mix[s].start()

    def B(s):
        mix[s].b()

    def C(s):
        mix[s].c()

    def D(s):
        M[h.c, h.y, pl.ds(s * LEN, LEN), :] = mix[s].d().astype(BF16)
        mids[s].t0()

    def E(s):
        mids[s].t1()

    def F(s):
        mids[s].t2()

    def G(s):
        mids[s].t3()

        def tile(i, carry):
            rows = pl.ds(pl.multiple_of(s * LEN + i * 16, 16), 16)
            mixed = whole(M, rows)
            factor = mean_factor(total(mixed))
            pieces = []
            for j in range(8):
                r = X[j % 2, j // 2, rows, :].astype(F32) + mixed[j] * factor * gain(1, j)
                r = r.astype(BF16)
                X[j % 2, j // 2, rows, :] = r
                pieces.append(r.astype(F32))
            factor = mean_factor(total(pieces))
            for j in range(8):
                N[rows, j * W : (j + 1) * W] = (pieces[j] * factor * gain(2, j)).astype(BF16)
            return carry

        lax.fori_loop(0, LEN // 16, tile, 0)
        rows = pl.ds(s * LEN, LEN)
        lifted = jnp.dot(N[rows, :], WU[...].reshape(8 * W, 4 * W), preferred_element_type=F32)
        lifted = jnp.maximum(lifted, 0.0)
        ACT[rows, :] = (lifted * lifted).astype(BF16)

    def H(s):
        spread(ACT[pl.ds(s * LEN, LEN), :], WD, PB, s)
        ffn[s].start()

    def D2(s):
        own = ffn[s].d()
        OWN[pl.ds(s * LEN, LEN), :] = own
        ST[h.col, s : s + 1, :] = jnp.sum((own * own).T, axis=0, keepdims=True)

    loads[0].wait()
    toks[0].t0()
    toks[1].t0()
    for load in loads[1:4]:
        load.wait()
    bcv.p1()
    loads[4].wait()
    outw.p1()
    loads[5].wait()
    up.p1()
    loads[6].wait()
    ST[h.col] = jnp.zeros((8, W), F32)

    bcv.s1()
    outw.s1()
    bcv.s2()
    toks[0].t1()
    outw.s2()
    toks[1].t1()
    bcv.s3()
    up.s1()
    toks[0].t2()
    outw.s3()
    toks[0].t3()
    norm_tokens(0, 512)
    toks[1].t2()
    toks[1].t3()
    norm_tokens(512, 512)
    bcv.s4()
    A(0, outw.s4)
    up.s2()
    down.p1()
    B(0)
    A(1)
    C(0)
    B(1)
    A(2)
    down.s1()
    D(0)
    C(1)
    B(2)
    A(3)
    up.s3()
    E(0)
    D(1)
    C(2)
    B(3)
    down.s2()
    F(0)
    E(1)
    D(2)
    C(3)
    F(1)
    E(2)
    D(3)
    early.drain()
    up.s4()
    G(0)
    F(2)
    E(3)
    down.s3()
    G(1)
    F(3)
    G(2)
    G(3)
    down.s4()
    H(0)
    ffn[0].b()
    H(1)
    ffn[0].c()
    ffn[1].b()
    H(2)
    D2(0)
    ffn[1].c()
    ffn[2].b()
    H(3)
    D2(1)
    ffn[2].c()
    ffn[3].b()
    D2(2)
    ffn[3].c()
    D2(3)

    waits = []
    for dy, dc, dev in peers:
        source = lax.rem(h.y + 4 - dy, 4) * 2 + lax.rem(h.c + 2 - dc, 2)
        waits.append(link.same(ST.at[h.col], ST.at[source], dev))
    for wait in waits:
        wait()
    factors = mean_factor(sum(ST[k] for k in range(8)))
    for s in range(NSEQ):
        rows = pl.ds(s * LEN, LEN)
        wide = jnp.broadcast_to(factors[s : s + 1, :], (128, LEN)).T
        wide = jnp.concatenate([wide, wide], axis=1)
        closing = OWN[rows, :] * wide * consts[3:4, own_cols]
        out[rows, :] = (X[h.c, h.y, rows, :].astype(F32) + closing).astype(BF16)
    link.drain()


def body(
    tokens, mix_in_gain, bgate_weight, cgate_weight, value_weight, conv_taps, out_weight,
    mix_out_gain, ffn_in_gain, up_weight, down_weight, ffn_out_gain,
):
    gains = jnp.stack([mix_in_gain, mix_out_gain, ffn_in_gain, ffn_out_gain])
    consts = jnp.concatenate([gains, conv_taps, conv_taps[:1]]).astype(F32)
    hbm = pl.BlockSpec(memory_space=pl.ANY)
    vmem = pl.BlockSpec(memory_space=pltpu.VMEM)
    reduce_scratch = [
        pltpu.VMEM((2, 4, ROWS, W), BF16),
        pltpu.VMEM((4, ROWS, W), BF16),
        pltpu.VMEM((2, NSEQ, LEN // 2, W), BF16),
        pltpu.VMEM((2, ROWS, W), BF16),
    ]
    return pl.pallas_call(
        kernel,
        out_shape=jax.ShapeDtypeStruct((ROWS, W), BF16),
        in_specs=[hbm] * 7 + [vmem],
        out_specs=vmem,
        scratch_shapes=[
            pltpu.VMEM((2, 4, ROWS, W), BF16),
            pltpu.VMEM((2, 4, ROWS, W), BF16),
            pltpu.VMEM((ROWS, 8 * W), BF16),
            pltpu.VMEM((4, 512, 3 * W), BF16),
            pltpu.VMEM((4, W, 512), BF16),
            pltpu.VMEM((4, 512, 4 * W), BF16),
            pltpu.VMEM((4, 4 * W, 512), BF16),
            pltpu.VMEM((ROWS, 4 * W), BF16),
            *reduce_scratch,
            *reduce_scratch,
            pltpu.VMEM((ROWS, W), F32),
            pltpu.VMEM((8, 8, W), F32),
            pltpu.SemaphoreType.DMA((NSEM,)),
            pltpu.SemaphoreType.DMA((NSEM,)),
            pltpu.SemaphoreType.DMA((7,)),
        ],
        compiler_params=pltpu.CompilerParams(
            collective_id=0, has_side_effects=True, vmem_limit_bytes=64 * 1024 * 1024 - 65536
        ),
    )(tokens, bgate_weight, cgate_weight, value_weight, out_weight, up_weight, down_weight, consts)


def solution(mesh):
    torus = Mesh(mesh.devices.reshape(2, 4, 4, 4, 2), ("r", "z", "x", "y", "c"))
    fs, tp = ("z", "x"), ("y", "c")
    return jax.shard_map(
        body,
        mesh=torus,
        in_specs=(
            P(("r", "z", "x"), tp), P(), P(fs, tp), P(fs, tp), P(fs, tp), P(), P(tp, fs),
            P(), P(), P(fs, tp), P(tp, fs), P(),
        ),
        out_specs=P(("r", "z", "x"), tp),
        check_vma=False,
    )
```

```python
import jax
import jax.numpy as jnp
from jax import lax
from jax.experimental import pallas as pl
from jax.experimental.pallas import tpu as pltpu
from jax.sharding import Mesh
from jax.sharding import PartitionSpec as P

EPS = 1e-6
F32 = jnp.float32
BF16 = jnp.bfloat16
LEN = 256
ROWS = 1024
W = 256
NSEQ = ROWS // LEN
NSEND, NRECV = 9, 112
TILE = 64


class Link:
    def __init__(self, send, recv):
        self.send, self.recv, self.sends, self.recvs = send, recv, 0, 0

    def sender(self):
        self.sends += 1
        return self.send.at[self.sends - 1]

    def arrivals(self, n):
        first = self.recvs
        self.recvs += n
        return [self.recv.at[first + k] for k in range(n)]


def copy_of(src, dst, sent, got, device):
    return pltpu.make_async_remote_copy(
        src_ref=src, dst_ref=dst, send_sem=sent, recv_sem=got,
        device_id=device, device_id_type=pl.DeviceIdType.MESH,
    )


class Here:
    def __init__(self):
        r, z, x, y, c = (lax.axis_index(n) for n in ("r", "z", "x", "y", "c"))
        self.z, self.x, self.y, self.c = z, x, y, c
        plus = lambda v, k, n: lax.rem(v + k, n)
        self.xp, self.xo, self.xm = (plus(x, k, 4) for k in (1, 2, 3))
        self.yp, self.yo, self.ym = (plus(y, k, 4) for k in (1, 2, 3))
        self.zp, self.zo, self.zm = (plus(z, k, 4) for k in (1, 2, 3))
        self.cn = 1 - c
        up, down = plus(r * 4 + z, 1, 8), plus(r * 4 + z, 7, 8)
        self.to_xp, self.to_xm = {"x": self.xp}, {"x": self.xm}
        self.to_yp, self.to_ym = {"y": self.yp}, {"y": self.ym}
        self.to_zp = {"r": up // 4, "z": lax.rem(up, 4)}
        self.to_zm = {"r": down // 4, "z": lax.rem(down, 4)}
        self.to_mate = {"c": self.cn}
        self.col = y * 2 + c


def at128(v, n=128):
    return pl.ds(pl.multiple_of(v * 128, 128), n)


class Group:
    def __init__(self, link, here):
        self.h, self.sent = here, link.sender()

    def go(self, src, dst, got, device):
        copy_of(src, dst, self.sent, got, device).start()

    def same(self, mine, got, device):
        self.go(mine, mine, got, device)

    def landed(self, ref, got):
        copy_of(ref, ref, self.sent, got, self.h.to_mate).wait_recv()

    def drain(self, ref):
        copy_of(ref, ref, self.sent, self.sent, self.h.to_mate).wait_send()


class Weight:
    def __init__(self, link, here, buf, by_row):
        self.h, self.buf, self.by_row = here, buf, by_row
        self.half = (buf.shape[2] if by_row else buf.shape[1]) // 2
        self.g = Group(link, here)
        self.r1, self.r2 = link.arrivals(4), link.arrivals(1)[0]
        self.rf, self.rg = link.arrivals(4), link.arrivals(1)[0]

    def unit(self, z, x, part, half=None):
        if self.by_row:
            start, n = (0, 128) if half is None else (64 * half, 64)
            rows = pl.ds(pl.multiple_of(x * 128 + start, 64), n)
            return self.buf.at[z, rows, pl.ds(part * self.half, self.half)]
        q = self.half // 2
        rows = pl.ds(part * self.half, self.half) if half is None else pl.ds(part * self.half + half * q, q)
        return self.buf.at[z, rows, at128(x)]

    def line_a(self, z, half):
        if self.by_row:
            return self.buf.at[z, pl.ds(256 * half, 256), pl.ds(0, self.half)]
        q = self.half // 2
        return self.buf.at[z, pl.ds(q * half, q), :]

    def line_b(self, x, half):
        if self.by_row:
            return self.buf.at[pl.ds(2 * half, 2), at128(x), pl.ds(self.half, self.half)]
        return self.buf.at[pl.ds(2 * half, 2), pl.ds(self.half, self.half), at128(x)]

    def p1(self):
        h, s = self.h, self.g.same
        a, b = self.unit(h.z, h.x, 0), self.unit(h.z, h.x, 1)
        for src, got, dev in zip((a, a, b, b), self.r1, (h.to_xp, h.to_xm, h.to_zp, h.to_zm)):
            s(src, got, dev)

    def s1(self):
        h, u = self.h, self.unit
        for k, (at, dev) in enumerate((
            ((h.z, h.xm, 0), h.to_xp), ((h.z, h.xp, 0), h.to_xm),
            ((h.zm, h.x, 1), h.to_zp), ((h.zp, h.x, 1), h.to_zm),
        )):
            self.g.landed(u(*at), self.r1[k])
            self.g.same(u(*at, k % 2), self.r2, dev)

    def s2(self):
        h, s, a, b = self.h, self.g.same, self.line_a, self.line_b
        quarters = (
            self.buf.at[0, pl.ds(0, 256), pl.ds(0, self.half)] if self.by_row
            else self.buf.at[0, pl.ds(0, self.half), pl.ds(0, 256)]
        )
        self.g.landed(quarters, self.r2)
        s(a(h.z, 0), self.rf[0], h.to_zp)
        s(a(h.z, 1), self.rf[1], h.to_zm)
        s(b(h.x, 0), self.rf[2], h.to_xp)
        s(b(h.x, 1), self.rf[3], h.to_xm)
        s(a(h.z, 1), self.rg, h.to_zp)
        s(a(h.z, 0), self.rg, h.to_zm)
        s(b(h.x, 1), self.rg, h.to_xp)
        s(b(h.x, 0), self.rg, h.to_xm)

    def s3(self):
        h, a, b = self.h, self.line_a, self.line_b
        for k, (ref, dev) in enumerate((
            (a(h.zm, 0), h.to_zp), (a(h.zp, 1), h.to_zm), (b(h.xm, 0), h.to_xp), (b(h.xp, 1), h.to_xm),
        )):
            self.g.landed(ref, self.rf[k])
            self.g.same(ref, self.rg, dev)

    def s4(self):
        self.g.landed(self.buf.at[pl.ds(0, 2)], self.rg)

    def drain(self):
        self.g.drain(self.buf.at[:, pl.ds(0, self.buf.shape[1] // 16 * 15), :])


class Gather:
    def __init__(self, link, group, buf, row, n):
        self.s, self.h, self.buf, self.row, self.n = group, group.h, buf, row, n
        self.f, self.g = link.arrivals(2), link.arrivals(2)
        self.far, self.mate = link.arrivals(2)

    def piece(self, c, y, half=None):
        if half is None:
            return self.buf.at[c, y, pl.ds(self.row, self.n)]
        return self.buf.at[c, y, pl.ds(self.row + half * (self.n // 2), self.n // 2)]

    def t0(self):
        h, s, p = self.h, self.s.same, self.piece
        c, y = h.c, h.y
        s(p(c, y, 0), self.f[0], h.to_yp)
        s(p(c, y, 1), self.f[1], h.to_ym)
        s(p(c, y, 1), self.g[0], h.to_yp)
        s(p(c, y, 0), self.g[1], h.to_ym)
        s(p(c, y), self.mate, h.to_mate)

    def t1(self):
        h, s, p = self.h, self.s.same, self.piece
        c, got = h.c, self.s.landed
        for k, y, dev in ((0, h.ym, h.to_yp), (1, h.yp, h.to_ym)):
            got(p(c, y, k), self.f[k])
            s(p(c, y, k), self.far, dev)
        for k, y in ((0, h.ym), (1, h.yp)):
            got(p(c, y, 1 - k), self.g[k])
            s(p(c, y), self.mate, h.to_mate)

    def t2(self):
        h, p = self.h, self.piece
        self.s.landed(p(h.c, h.yo), self.far)
        self.s.same(p(h.c, h.yo), self.mate, h.to_mate)

    def t3(self):
        self.s.landed(self.buf.at[self.h.cn, :, pl.ds(self.row, self.n)], self.mate)


class Reduce:
    def __init__(self, link, group, part, mate, r1, r2, seq):
        self.s, self.h, self.part, self.mate, self.r1, self.r2 = group, group.h, part, mate, r1, r2
        self.seq, self.row = seq, seq * LEN
        self.w0, self.w1, self.w2 = link.arrivals(1)[0], link.arrivals(2), link.arrivals(1)[0]

    def start(self):
        h, rows = self.h, pl.ds(self.row, LEN)
        self.s.go(self.part.at[h.cn, :, rows], self.mate.at[:, rows], self.w0, h.to_mate)

    def both(self, y, lo=0, n=LEN):
        rows = pl.ds(self.row + lo, n)
        return self.part[self.h.c, y, rows, :].astype(F32) + self.mate[y, rows, :].astype(F32)

    def b(self):
        h, half = self.h, LEN // 2
        self.s.landed(self.mate.at[:, pl.ds(self.row, LEN)], self.w0)
        for k, dev in ((0, h.to_yp), (1, h.to_ym)):
            rows = pl.ds(self.row + k * half, half)
            self.part[h.c, h.yo, rows, :] = self.both(h.yo, k * half, half).astype(BF16)
            self.s.go(self.part.at[h.c, h.yo, rows], self.r1.at[k, self.seq], self.w1[k], dev)

    def c(self):
        h, half = self.h, LEN // 2
        rows = pl.ds(self.row, LEN)
        for k, y, dev in ((0, h.yp, h.to_yp), (1, h.ym, h.to_ym)):
            self.s.landed(self.r1.at[k, self.seq], self.w1[k])
            add = self.r1[k, self.seq].astype(F32)
            near, far = self.both(y, k * half, half) + add, self.both(y, (1 - k) * half, half)
            self.part[h.c, y, pl.ds(self.row + k * half, half), :] = near.astype(BF16)
            self.part[h.c, y, pl.ds(self.row + (1 - k) * half, half), :] = far.astype(BF16)
            self.s.go(self.part.at[h.c, y, rows], self.r2.at[k, rows], self.w2, dev)

    def d(self):
        rows = pl.ds(self.row, LEN)
        self.s.landed(self.r2.at[:, rows], self.w2)
        return self.both(self.h.y) + self.r2[0, rows, :].astype(F32) + self.r2[1, rows, :].astype(F32)


def mean_factor(total):
    return lax.rsqrt(total * (1.0 / (8 * W)) + EPS)


def kernel(
    tok, bw, cw, vw, ow, uw, dw, g0, g1, g2, g3, taps3, out,
    consts, ga, gb, gc, gd, taps, X, M, N, WB, WO, WU, WD, ACT, PA, RDA, R1A, R2A, PB, RDB, R1B, R2B, OWN, ST,
    send, recv, local,
):
    h = Here()
    link = Link(send, recv)
    early, late, sums, last, stats = (Group(link, h) for _ in range(5))
    own_rows = at128(h.x)
    loads = [
        pltpu.make_async_copy(tok, X.at[h.c, h.y], local.at[0]),
        pltpu.make_async_copy(bw, WB.at[h.z, own_rows, pl.ds(0, W)], local.at[1]),
        pltpu.make_async_copy(cw, WB.at[h.z, own_rows, pl.ds(W, W)], local.at[2]),
        pltpu.make_async_copy(vw, WB.at[h.z, own_rows, pl.ds(2 * W, W)], local.at[3]),
        pltpu.make_async_copy(ow, WO.at[h.z, :, own_rows], local.at[4]),
        pltpu.make_async_copy(uw, WU.at[h.z, own_rows, :], local.at[5]),
        pltpu.make_async_copy(dw, WD.at[h.z, :, own_rows], local.at[6]),
    ] + [
        pltpu.make_async_copy(src, dst, local.at[7 + k])
        for k, (src, dst) in enumerate(((g0, ga), (g1, gb), (g2, gc), (g3, gd), (taps3, taps)))
    ]
    for load in loads:
        load.start()

    peers = [
        {"y": lax.rem(h.y + dy, 4), "c": lax.rem(h.c + dc, 2)}
        for dy in range(4) for dc in range(2) if dy or dc
    ]
    barrier = pltpu.get_barrier_semaphore()
    targets = [h.to_xp, h.to_xm, h.to_zp, h.to_zm] + peers
    for dev in targets:
        pl.semaphore_signal(barrier, inc=1, device_id=dev, device_id_type=pl.DeviceIdType.MESH)
    pl.semaphore_wait(barrier, len(targets))

    toks = [Gather(link, early, X, t * 512, 512) for t in range(2)]
    bcv, outw = Weight(link, h, WB, True), Weight(link, h, WO, False)
    up, down = Weight(link, h, WU, True), Weight(link, h, WD, False)
    mix = [Reduce(link, sums, PA, RDA, R1A, R2A, s) for s in range(NSEQ)]
    ffn = [Reduce(link, last, PB, RDB, R1B, R2B, s) for s in range(NSEQ)]
    mids = [Gather(link, late, M, s * LEN, LEN) for s in range(NSEQ)]

    def total(pieces):
        squares = sum(p * p for p in pieces)
        return jnp.sum(squares, axis=1, keepdims=True)

    def gain(k, j):
        return consts[k : k + 1, j * W : (j + 1) * W]

    def blocks(buf, rows):
        return [buf.at[j % 2, j // 2, rows, :] for j in range(8)]

    def scale_out(source, rows, which):
        factor = mean_factor(total([ref[...].astype(F32) for ref in blocks(source, rows)]))
        for j, ref in enumerate(blocks(source, rows)):
            N[rows, j * W : (j + 1) * W] = (ref[...].astype(F32) * factor * gain(which, j)).astype(BF16)

    def norm_tokens(first, count):
        def tile(i, carry):
            scale_out(X, pl.ds(pl.multiple_of(first + i * TILE, TILE), TILE), 0)
            return carry

        lax.fori_loop(0, count // TILE, tile, 0)

    position = lax.broadcasted_iota(jnp.int32, (LEN, W), 0)
    own_cols = pl.ds(pl.multiple_of(h.col * W, W), W)

    def mixer(s):
        rows = pl.ds(s * LEN, LEN)
        three = jnp.dot(N[rows, :], WB[...].reshape(8 * W, 3 * W), preferred_element_type=F32)
        b, c, v = (three[:, k * W : (k + 1) * W].astype(BF16).astype(F32) for k in range(3))
        inner = c * v
        before = jnp.where(position == 0, 0.0, pltpu.roll(inner, 1, 0))
        after = jnp.where(position == LEN - 1, 0.0, pltpu.roll(inner, LEN - 1, 0))
        tap = [consts[4 + k : 5 + k, own_cols] for k in range(3)]
        conv = tap[0] * before + tap[1] * inner + tap[2] * after
        return (b * conv).astype(BF16)

    def spread(left, weight, part, s):
        rows = pl.ds(s * LEN, LEN)
        for y in range(4):
            piece = jnp.dot(left, weight[y], preferred_element_type=F32).astype(BF16)
            part[0, y, rows, :] = piece[:, :W]
            part[1, y, rows, :] = piece[:, W:]

    def A(s, before_out=None):
        gated = mixer(s)
        if before_out:
            before_out()
        spread(gated, WO, PA, s)
        mix[s].start()

    def B(s):
        mix[s].b()

    def C(s):
        mix[s].c()

    def D(s):
        M[h.c, h.y, pl.ds(s * LEN, LEN), :] = mix[s].d().astype(BF16)
        mids[s].t0()

    def E(s):
        mids[s].t1()

    def F(s):
        mids[s].t2()

    def G(s):
        mids[s].t3()

        def tile(i, carry):
            rows = pl.ds(pl.multiple_of(s * LEN + i * TILE, TILE), TILE)
            mixed, kept = blocks(M, rows), blocks(X, rows)
            factor = mean_factor(total([ref[...].astype(F32) for ref in mixed]))
            for j in range(8):
                add = mixed[j][...].astype(F32) * factor * gain(1, j)
                kept[j][...] = (kept[j][...].astype(F32) + add).astype(BF16)
            scale_out(X, rows, 2)
            return carry

        lax.fori_loop(0, LEN // TILE, tile, 0)
        rows = pl.ds(s * LEN, LEN)
        lifted = jnp.dot(N[rows, :], WU[...].reshape(8 * W, 4 * W), preferred_element_type=F32)
        lifted = jnp.maximum(lifted, 0.0)
        ACT[rows, :] = (lifted * lifted).astype(BF16)

    def H(s):
        spread(ACT[pl.ds(s * LEN, LEN), :], WD, PB, s)
        ffn[s].start()

    def D2(s):
        own = ffn[s].d()
        OWN[pl.ds(s * LEN, LEN), :] = own
        energy = jnp.sum((own * own).T, axis=0, keepdims=True)
        ST[s, h.col] = jnp.broadcast_to(energy, (8, W))
        for dev in peers:
            stats.same(ST.at[s, h.col], known[s], dev)

    def finish(s):
        stats.landed(ST.at[s, pl.ds(0, 7)], known[s])
        factor = mean_factor(sum(ST[s, k] for k in range(8)))
        rows = pl.ds(s * LEN, LEN)
        wide = jnp.broadcast_to(factor[:1, :], (128, LEN)).T
        wide = jnp.concatenate([wide, wide], axis=1)
        closing = OWN[rows, :] * wide * consts[3:4, own_cols]
        out[rows, :] = (X[h.c, h.y, rows, :].astype(F32) + closing).astype(BF16)

    known = link.arrivals(NSEQ)

    loads[0].wait()
    toks[0].t0()
    toks[1].t0()
    for load in loads[1:4]:
        load.wait()
    bcv.p1()
    loads[4].wait()
    outw.p1()
    loads[5].wait()
    up.p1()
    loads[6].wait()
    for load in loads[7:]:
        load.wait()
    for k, g in enumerate((ga, gb, gc, gd)):
        consts[k : k + 1, :] = g[...].astype(F32)[None, :]
    consts[4:7, :] = taps[...].astype(F32)

    bcv.s1()
    outw.s1()
    bcv.s2()
    toks[0].t1()
    outw.s2()
    toks[1].t1()
    toks[0].t2()
    bcv.s3()
    toks[0].t3()
    norm_tokens(0, 512)
    toks[1].t2()
    outw.s3()
    up.s1()
    down.p1()
    toks[1].t3()
    norm_tokens(512, 512)
    bcv.s4()
    A(0, outw.s4)
    up.s2()
    A(1)
    B(0)
    A(2)
    B(1)
    C(0)
    down.s1()
    A(3)
    B(2)
    C(1)
    D(0)
    up.s3()
    B(3)
    C(2)
    D(1)
    down.s2()
    E(0)
    C(3)
    D(2)
    E(1)
    early.drain(X.at[:, :, pl.ds(0, 896)])
    F(0)
    D(3)
    down.s3()
    up.s4()
    G(0)
    E(2)
    F(1)
    E(3)
    F(2)
    G(1)
    F(3)
    down.s4()
    H(0)
    G(2)
    ffn[0].b()
    H(1)
    G(3)
    ffn[1].b()
    ffn[0].c()
    H(2)
    H(3)
    ffn[2].b()
    ffn[1].c()
    D2(0)
    ffn[3].b()
    ffn[2].c()
    D2(1)
    finish(0)
    ffn[3].c()
    D2(2)
    finish(1)
    D2(3)
    finish(2)
    finish(3)
    late.drain(M.at[:, :, pl.ds(0, 896)])
    sums.drain(PA.at[:, :, pl.ds(0, 896)])
    last.drain(PB.at[:, :, pl.ds(0, 896)])
    stats.drain(ST.at[:, pl.ds(0, 7)])
    for weight in (bcv, outw, up, down):
        weight.drain()


def body(
    tokens, mix_in_gain, bgate_weight, cgate_weight, value_weight, conv_taps, out_weight,
    mix_out_gain, ffn_in_gain, up_weight, down_weight, ffn_out_gain,
):
    hbm = pl.BlockSpec(memory_space=pltpu.HBM)
    vmem = pl.BlockSpec(memory_space=pltpu.VMEM)
    reduce_scratch = [
        pltpu.VMEM((2, 4, ROWS, W), BF16),
        pltpu.VMEM((4, ROWS, W), BF16),
        pltpu.VMEM((2, NSEQ, LEN // 2, W), BF16),
        pltpu.VMEM((2, ROWS, W), BF16),
    ]
    return pl.pallas_call(
        kernel,
        out_shape=jax.ShapeDtypeStruct((ROWS, W), BF16),
        in_specs=[hbm] * 12,
        out_specs=vmem,
        scratch_shapes=[
            pltpu.VMEM((8, 8 * W), F32),
            *[pltpu.VMEM((8 * W,), BF16)] * 4,
            pltpu.VMEM((3, 8 * W), BF16),
            pltpu.VMEM((2, 4, ROWS, W), BF16),
            pltpu.VMEM((2, 4, ROWS, W), BF16),
            pltpu.VMEM((ROWS, 8 * W), BF16),
            pltpu.VMEM((4, 512, 3 * W), BF16),
            pltpu.VMEM((4, W, 512), BF16),
            pltpu.VMEM((4, 512, 4 * W), BF16),
            pltpu.VMEM((4, 4 * W, 512), BF16),
            pltpu.VMEM((ROWS, 4 * W), BF16),
            *reduce_scratch,
            *reduce_scratch,
            pltpu.VMEM((ROWS, W), F32),
            pltpu.VMEM((NSEQ, 8, 8, W), F32),
            pltpu.SemaphoreType.DMA((NSEND,)),
            pltpu.SemaphoreType.DMA((NRECV,)),
            pltpu.SemaphoreType.DMA((12,)),
        ],
        compiler_params=pltpu.CompilerParams(
            collective_id=0, has_side_effects=True, vmem_limit_bytes=64 * 1024 * 1024 - 65536
        ),
    )(tokens, bgate_weight, cgate_weight, value_weight, out_weight, up_weight, down_weight,
      mix_in_gain, mix_out_gain, ffn_in_gain, ffn_out_gain, conv_taps)


def solution(mesh):
    torus = Mesh(mesh.devices.reshape(2, 4, 4, 4, 2), ("r", "z", "x", "y", "c"))
    fs, tp = ("z", "x"), ("y", "c")
    return jax.shard_map(
        body,
        mesh=torus,
        in_specs=(
            P(("r", "z", "x"), tp), P(), P(fs, tp), P(fs, tp), P(fs, tp), P(), P(tp, fs),
            P(), P(), P(fs, tp), P(tp, fs), P(),
        ),
        out_specs=P(("r", "z", "x"), tp),
        check_vma=False,
    )
```

```python
import jax
import jax.numpy as jnp
from jax import lax
from jax.experimental import pallas as pl
from jax.experimental.pallas import tpu as pltpu
from jax.sharding import Mesh
from jax.sharding import PartitionSpec as P

EPS = 1e-6
F32 = jnp.float32
BF16 = jnp.bfloat16
LEN = 256
ROWS = 1024
W = 256
NSEQ = ROWS // LEN
NSEND, NRECV = 9, 120
TILE = 64


class Link:
    def __init__(self, send, recv):
        self.send, self.recv, self.sends, self.recvs = send, recv, 0, 0

    def sender(self):
        self.sends += 1
        return self.send.at[self.sends - 1]

    def arrivals(self, n):
        first = self.recvs
        self.recvs += n
        return [self.recv.at[first + k] for k in range(n)]


def copy_of(src, dst, sent, got, device):
    return pltpu.make_async_remote_copy(
        src_ref=src, dst_ref=dst, send_sem=sent, recv_sem=got,
        device_id=device, device_id_type=pl.DeviceIdType.MESH,
    )


class Here:
    def __init__(self):
        r, z, x, y, c = (lax.axis_index(n) for n in ("r", "z", "x", "y", "c"))
        self.z, self.x, self.y, self.c = z, x, y, c
        plus = lambda v, k, n: lax.rem(v + k, n)
        self.xp, self.xo, self.xm = (plus(x, k, 4) for k in (1, 2, 3))
        self.yp, self.yo, self.ym = (plus(y, k, 4) for k in (1, 2, 3))
        self.zp, self.zo, self.zm = (plus(z, k, 4) for k in (1, 2, 3))
        self.cn = 1 - c
        up, down = plus(r * 4 + z, 1, 8), plus(r * 4 + z, 7, 8)
        self.to_xp, self.to_xm = {"x": self.xp}, {"x": self.xm}
        self.to_yp, self.to_ym = {"y": self.yp}, {"y": self.ym}
        self.to_zp = {"r": up // 4, "z": lax.rem(up, 4)}
        self.to_zm = {"r": down // 4, "z": lax.rem(down, 4)}
        self.to_mate = {"c": self.cn}
        self.col = y * 2 + c


def at128(v, n=128):
    return pl.ds(pl.multiple_of(v * 128, 128), n)


class Group:
    def __init__(self, link, here):
        self.h, self.sent = here, link.sender()

    def go(self, src, dst, got, device):
        copy_of(src, dst, self.sent, got, device).start()

    def same(self, mine, got, device):
        self.go(mine, mine, got, device)

    def landed(self, ref, got):
        copy_of(ref, ref, self.sent, got, self.h.to_mate).wait_recv()

    def drain(self, ref):
        copy_of(ref, ref, self.sent, self.sent, self.h.to_mate).wait_send()


class Weight:
    def __init__(self, link, here, buf, by_row):
        self.h, self.buf, self.by_row = here, buf, by_row
        self.half = (buf.shape[2] if by_row else buf.shape[1]) // 2
        self.g = Group(link, here)
        self.r1, self.r2 = link.arrivals(4), link.arrivals(1)[0]
        self.rf, self.rg = link.arrivals(4), link.arrivals(1)[0]

    def unit(self, z, x, part, half=None):
        if self.by_row:
            start, n = (0, 128) if half is None else (64 * half, 64)
            rows = pl.ds(pl.multiple_of(x * 128 + start, 64), n)
            return self.buf.at[z, rows, pl.ds(part * self.half, self.half)]
        q = self.half // 2
        rows = pl.ds(part * self.half, self.half) if half is None else pl.ds(part * self.half + half * q, q)
        return self.buf.at[z, rows, at128(x)]

    def neighbours(self):
        h = self.h
        return (
            ((h.z, h.xm, 0), h.to_xp), ((h.z, h.xp, 0), h.to_xm),
            ((h.zm, h.x, 1), h.to_zp), ((h.zp, h.x, 1), h.to_zm),
        )

    def p1(self, early):
        h = self.h
        for k, (_, dev) in enumerate(self.neighbours()):
            half = k % 2 if early else 1 - k % 2
            self.g.same(self.unit(h.z, h.x, k // 2, half), self.r1[k] if early else self.r2, dev)

    def s1(self):
        for k, (at, dev) in enumerate(self.neighbours()):
            ref = self.unit(*at, k % 2)
            self.g.landed(ref, self.r1[k])
            self.g.same(ref, self.r2, dev)

    def second(self):
        h, u = self.h, self.unit
        a = [lambda z, x=x: u(z, x, 0) for x in (h.x, h.xp, h.xo, h.xm)]
        b = [lambda x, z=z: u(z, x, 1) for z in (h.z, h.zp, h.zo, h.zm)]
        return (
            (a, h.z, h.zm, (0, 1), (2, 3), h.to_zp), (a, h.z, h.zp, (2, 3), (0, 1), h.to_zm),
            (b, h.x, h.xm, (0, 1), (2, 3), h.to_xp), (b, h.x, h.xp, (2, 3), (0, 1), h.to_xm),
        )

    def own2(self):
        for k, (line, here, _, passed, _, dev) in enumerate(self.second()):
            self.g.same(line[0](here), self.rf[k] if 0 in passed else self.rg, dev)

    def s2(self):
        if self.by_row:
            self.g.landed(self.buf.at[0, :, pl.ds(0, self.half)], self.r2)
        else:
            self.g.landed(self.buf.at[0, pl.ds(0, self.half), :], self.r2)
        for first in (True, False):
            for k, (line, here, _, passed, kept, dev) in enumerate(self.second()):
                for n in passed if first else kept:
                    if n:
                        self.g.same(line[n](here), self.rf[k] if first else self.rg, dev)

    def s3(self):
        two = (
            self.buf.at[0, pl.ds(0, 256), pl.ds(0, self.half)] if self.by_row
            else self.buf.at[0, pl.ds(0, self.half), pl.ds(0, 256)]
        )
        for k, (line, _, source, passed, _, dev) in enumerate(self.second()):
            self.g.landed(two, self.rf[k])
            for n in passed:
                self.g.same(line[n](source), self.rg, dev)

    def s4(self):
        self.g.landed(self.buf.at[pl.ds(0, 2)], self.rg)

    def drain(self):
        self.g.drain(self.buf.at[:, pl.ds(0, self.buf.shape[1] // 16 * 15), :])


class Gather:
    def __init__(self, link, group, buf, row, n):
        self.s, self.h, self.buf, self.row, self.n = group, group.h, buf, row, n
        self.f, self.g = link.arrivals(2), link.arrivals(2)
        self.far, self.mate = link.arrivals(2)

    def piece(self, c, y, half=None):
        if half is None:
            return self.buf.at[c, y, pl.ds(self.row, self.n)]
        return self.buf.at[c, y, pl.ds(self.row + half * (self.n // 2), self.n // 2)]

    def t0(self):
        h, s, p = self.h, self.s.same, self.piece
        c, y = h.c, h.y
        s(p(c, y, 0), self.f[0], h.to_yp)
        s(p(c, y, 1), self.f[1], h.to_ym)
        s(p(c, y, 1), self.g[0], h.to_yp)
        s(p(c, y, 0), self.g[1], h.to_ym)
        s(p(c, y), self.mate, h.to_mate)

    def t1(self):
        h, s, p = self.h, self.s.same, self.piece
        c, got = h.c, self.s.landed
        for k, y, dev in ((0, h.ym, h.to_yp), (1, h.yp, h.to_ym)):
            got(p(c, y, k), self.f[k])
            s(p(c, y, k), self.far, dev)

    def t1b(self):
        h, s, p = self.h, self.s.same, self.piece
        c, got = h.c, self.s.landed
        for k, y in ((0, h.ym), (1, h.yp)):
            got(p(c, y, 1 - k), self.g[k])
            s(p(c, y), self.mate, h.to_mate)

    def t2(self):
        h, p = self.h, self.piece
        self.s.landed(p(h.c, h.yo), self.far)
        self.s.same(p(h.c, h.yo), self.mate, h.to_mate)

    def t3(self):
        self.s.landed(self.buf.at[self.h.cn, :, pl.ds(self.row, self.n)], self.mate)


class Reduce:
    def __init__(self, link, group, part, mate, r1, r2, seq):
        self.s, self.h, self.part, self.mate, self.r1, self.r2 = group, group.h, part, mate, r1, r2
        self.seq, self.row = seq, seq * LEN
        self.w0, self.w1, self.w2 = link.arrivals(2), link.arrivals(2), link.arrivals(1)[0]

    def start(self, y, k):
        h, rows = self.h, pl.ds(self.row, LEN)
        self.s.go(self.part.at[h.cn, y, rows], self.mate.at[y, rows], self.w0[k], h.to_mate)

    def both(self, y, lo=0, n=LEN):
        rows = pl.ds(self.row + lo, n)
        return self.part[self.h.c, y, rows, :].astype(F32) + self.mate[y, rows, :].astype(F32)

    def b(self):
        h, half = self.h, LEN // 2
        self.s.landed(self.mate.at[h.yo, pl.ds(self.row, LEN)], self.w0[0])
        for k, dev in ((0, h.to_yp), (1, h.to_ym)):
            rows = pl.ds(self.row + k * half, half)
            self.part[h.c, h.yo, rows, :] = self.both(h.yo, k * half, half).astype(BF16)
            self.s.go(self.part.at[h.c, h.yo, rows], self.r1.at[k, self.seq], self.w1[k], dev)

    def c(self):
        h, half = self.h, LEN // 2
        rows = pl.ds(self.row, LEN)
        self.s.landed(self.mate.at[pl.ds(0, 3), rows], self.w0[1])
        for k, y, dev in ((0, h.yp, h.to_yp), (1, h.ym, h.to_ym)):
            self.s.landed(self.r1.at[k, self.seq], self.w1[k])
            add = self.r1[k, self.seq].astype(F32)
            near, far = self.both(y, k * half, half) + add, self.both(y, (1 - k) * half, half)
            self.part[h.c, y, pl.ds(self.row + k * half, half), :] = near.astype(BF16)
            self.part[h.c, y, pl.ds(self.row + (1 - k) * half, half), :] = far.astype(BF16)
            self.s.go(self.part.at[h.c, y, rows], self.r2.at[k, rows], self.w2, dev)

    def d(self):
        rows = pl.ds(self.row, LEN)
        self.s.landed(self.r2.at[:, rows], self.w2)
        return self.both(self.h.y) + self.r2[0, rows, :].astype(F32) + self.r2[1, rows, :].astype(F32)


def mean_factor(total):
    return lax.rsqrt(total * (1.0 / (8 * W)) + EPS)


def kernel(
    tok, bw, cw, vw, ow, uw, dw, g0, g1, g2, g3, taps3, out,
    consts, ga, gb, gc, gd, taps, X, M, N, WB, WO, WU, WD, ACT, PA, RDA, R1A, R2A, PB, RDB, R1B, R2B, OWN, ST, OUTV,
    send, recv, local,
):
    h = Here()
    link = Link(send, recv)
    early, late, sums, last, stats = (Group(link, h) for _ in range(5))
    own_rows = at128(h.x)
    loads = [
        pltpu.make_async_copy(tok, X.at[h.c, h.y], local.at[0]),
        pltpu.make_async_copy(bw, WB.at[h.z, own_rows, pl.ds(0, W)], local.at[1]),
        pltpu.make_async_copy(cw, WB.at[h.z, own_rows, pl.ds(W, W)], local.at[2]),
        pltpu.make_async_copy(vw, WB.at[h.z, own_rows, pl.ds(2 * W, W)], local.at[3]),
        pltpu.make_async_copy(ow, WO.at[h.z, :, own_rows], local.at[4]),
        pltpu.make_async_copy(uw, WU.at[h.z, own_rows, :], local.at[5]),
        pltpu.make_async_copy(dw, WD.at[h.z, :, own_rows], local.at[6]),
    ] + [
        pltpu.make_async_copy(src, dst, local.at[7 + k])
        for k, (src, dst) in enumerate(((g0, ga), (g1, gb), (g2, gc), (g3, gd), (taps3, taps)))
    ]
    for load in loads:
        load.start()

    peers = [
        {"y": lax.rem(h.y + dy, 4), "c": lax.rem(h.c + dc, 2)}
        for dy in range(4) for dc in range(2) if dy or dc
    ]
    barrier = pltpu.get_barrier_semaphore()
    targets = [h.to_xp, h.to_xm, h.to_zp, h.to_zm] + peers
    for dev in targets:
        pl.semaphore_signal(barrier, inc=1, device_id=dev, device_id_type=pl.DeviceIdType.MESH)
    pl.semaphore_wait(barrier, len(targets))

    toks = [Gather(link, early, X, t * 512, 512) for t in range(2)]
    bcv, outw = Weight(link, h, WB, True), Weight(link, h, WO, False)
    up, down = Weight(link, h, WU, True), Weight(link, h, WD, False)
    mix = [Reduce(link, sums, PA, RDA, R1A, R2A, s) for s in range(NSEQ)]
    ffn = [Reduce(link, last, PB, RDB, R1B, R2B, s) for s in range(NSEQ)]
    mids = [Gather(link, late, M, s * LEN, LEN) for s in range(NSEQ)]

    def total(pieces):
        squares = sum(p * p for p in pieces)
        return jnp.sum(squares, axis=1, keepdims=True)

    def gain(k, j):
        return consts[k : k + 1, j * W : (j + 1) * W]

    def blocks(buf, rows):
        return [buf.at[j % 2, j // 2, rows, :] for j in range(8)]

    def scale_out(source, rows, which):
        factor = mean_factor(total([ref[...].astype(F32) for ref in blocks(source, rows)]))
        for j, ref in enumerate(blocks(source, rows)):
            N[rows, j * W : (j + 1) * W] = (ref[...].astype(F32) * factor * gain(which, j)).astype(BF16)

    def norm_tokens(first, count):
        def tile(i, carry):
            scale_out(X, pl.ds(pl.multiple_of(first + i * TILE, TILE), TILE), 0)
            return carry

        lax.fori_loop(0, count // TILE, tile, 0)

    position = lax.broadcasted_iota(jnp.int32, (LEN, W), 0)
    own_cols = pl.ds(pl.multiple_of(h.col * W, W), W)

    def mixer(s):
        rows = pl.ds(s * LEN, LEN)
        three = jnp.dot(N[rows, :], WB[...].reshape(8 * W, 3 * W), preferred_element_type=F32)
        b, c, v = (three[:, k * W : (k + 1) * W].astype(BF16).astype(F32) for k in range(3))
        inner = c * v
        before = jnp.where(position == 0, 0.0, pltpu.roll(inner, 1, 0))
        after = jnp.where(position == LEN - 1, 0.0, pltpu.roll(inner, LEN - 1, 0))
        tap = [consts[4 + k : 5 + k, own_cols] for k in range(3)]
        conv = tap[0] * before + tap[1] * inner + tap[2] * after
        return (b * conv).astype(BF16)

    def spread(left, weight, part, reduce, eager):
        rows = pl.ds(reduce.row, LEN)
        order = (h.yo, h.yp, h.ym, h.y)
        for y in order if eager else range(4):
            piece = jnp.dot(left, weight[y], preferred_element_type=F32).astype(BF16)
            part[0, y, rows, :] = piece[:, :W]
            part[1, y, rows, :] = piece[:, W:]
            if eager:
                reduce.start(y, 0 if y is h.yo else 1)
        if not eager:
            for y in order:
                reduce.start(y, 0 if y is h.yo else 1)

    def A(s, before_out=None):
        gated = mixer(s)
        if before_out:
            before_out()
        spread(gated, WO, PA, mix[s], s == 0)

    def B(s):
        mix[s].b()

    def C(s):
        mix[s].c()

    def D(s):
        M[h.c, h.y, pl.ds(s * LEN, LEN), :] = mix[s].d().astype(BF16)
        mids[s].t0()

    def Ea(s):
        mids[s].t1()

    def Eb(s):
        mids[s].t1b()

    def F(s):
        mids[s].t2()

    def Ga(s):
        mids[s].t3()

        def tile(i, carry):
            rows = pl.ds(pl.multiple_of(s * LEN + i * TILE, TILE), TILE)
            mixed, kept = blocks(M, rows), blocks(X, rows)
            factor = mean_factor(total([ref[...].astype(F32) for ref in mixed]))
            for j in range(8):
                add = mixed[j][...].astype(F32) * factor * gain(1, j)
                kept[j][...] = (kept[j][...].astype(F32) + add).astype(BF16)
            scale_out(X, rows, 2)
            return carry

        lax.fori_loop(0, LEN // TILE, tile, 0)

    def Gb(s):
        rows = pl.ds(s * LEN, LEN)
        lifted = jnp.dot(N[rows, :], WU[...].reshape(8 * W, 4 * W), preferred_element_type=F32)
        lifted = jnp.maximum(lifted, 0.0)
        ACT[rows, :] = (lifted * lifted).astype(BF16)

    def H(s):
        spread(ACT[pl.ds(s * LEN, LEN), :], WD, PB, ffn[s], s == 0)

    def D2(s):
        own = ffn[s].d()
        OWN[pl.ds(s * LEN, LEN), :] = own
        energy = jnp.sum((own * own).T, axis=0, keepdims=True)
        ST[s, h.col] = energy
        for dev in peers:
            stats.same(ST.at[s, h.col], known[s], dev)

    def finish(s):
        stats.landed(ST.at[s, pl.ds(0, 7)], known[s])
        factor = mean_factor(sum(ST[s, k] for k in range(8)))
        rows = pl.ds(s * LEN, LEN)
        wide = jnp.broadcast_to(factor, (128, LEN)).T
        wide = jnp.concatenate([wide, wide], axis=1)
        closing = OWN[rows, :] * wide * consts[3:4, own_cols]
        OUTV[rows, :] = (X[h.c, h.y, rows, :].astype(F32) + closing).astype(BF16)
        stored.append(pltpu.make_async_copy(OUTV.at[rows], out.at[rows], local.at[12 + s]))
        stored[-1].start()

    known, stored = link.arrivals(NSEQ), []

    loads[0].wait()
    toks[0].t0()
    toks[1].t0()
    for load in loads[1:4]:
        load.wait()
    bcv.p1(True)
    bcv.p1(False)
    loads[4].wait()
    outw.p1(True)
    outw.p1(False)
    for load in loads[5:]:
        load.wait()
    for k, g in enumerate((ga, gb, gc, gd)):
        consts[k : k + 1, :] = g[...].astype(F32)[None, :]
    consts[4:7, :] = taps[...].astype(F32)

    bcv.s1()
    bcv.own2()
    up.p1(True)
    outw.s1()
    outw.own2()
    bcv.s2()
    outw.s2()
    toks[0].t1()
    toks[0].t1b()
    bcv.s3()
    toks[1].t1()
    toks[1].t1b()
    toks[0].t2()
    toks[0].t3()
    norm_tokens(0, 512)
    outw.s3()
    toks[1].t2()
    up.p1(False)
    up.s1()
    toks[1].t3()
    norm_tokens(512, 512)
    bcv.s4()
    up.own2()
    down.p1(True)
    down.p1(False)
    A(0, outw.s4)
    B(0)
    A(1)
    up.s2()
    B(1)
    C(0)
    A(2)
    B(2)
    C(1)
    down.s1()
    down.own2()
    A(3)
    B(3)
    D(0)
    up.s3()
    C(2)
    Ea(0)
    D(1)
    C(3)
    Eb(0)
    down.s2()
    F(0)
    Ea(1)
    D(2)
    Eb(1)
    early.drain(X.at[:, :, pl.ds(0, 896)])
    up.s4()
    Ga(0)
    Gb(0)
    F(1)
    down.s3()
    D(3)
    Ea(2)
    Eb(2)
    Ga(1)
    Ea(3)
    Gb(1)
    Eb(3)
    F(2)
    F(3)
    Ga(2)
    Gb(2)
    down.s4()
    H(0)
    ffn[0].b()
    H(1)
    H(2)
    ffn[1].b()
    ffn[0].c()
    ffn[2].b()
    Ga(3)
    Gb(3)
    ffn[1].c()
    H(3)
    ffn[3].b()
    D2(0)
    ffn[2].c()
    ffn[3].c()
    D2(1)
    D2(2)
    finish(0)
    D2(3)
    finish(1)
    finish(2)
    finish(3)
    late.drain(M.at[:, :, pl.ds(0, 896)])
    sums.drain(PA.at[:, :, pl.ds(0, 896)])
    last.drain(PB.at[:, :, pl.ds(0, 896)])
    stats.drain(ST.at[:, pl.ds(0, 7)])
    for weight in (bcv, outw, up, down):
        weight.drain()
    for copy in stored:
        copy.wait()


def body(
    tokens, mix_in_gain, bgate_weight, cgate_weight, value_weight, conv_taps, out_weight,
    mix_out_gain, ffn_in_gain, up_weight, down_weight, ffn_out_gain,
):
    hbm = pl.BlockSpec(memory_space=pltpu.HBM)
    reduce_scratch = [
        pltpu.VMEM((2, 4, ROWS, W), BF16),
        pltpu.VMEM((4, ROWS, W), BF16),
        pltpu.VMEM((2, NSEQ, LEN // 2, W), BF16),
        pltpu.VMEM((2, ROWS, W), BF16),
    ]
    return pl.pallas_call(
        kernel,
        out_shape=jax.ShapeDtypeStruct((ROWS, W), BF16),
        in_specs=[hbm] * 12,
        out_specs=hbm,
        scratch_shapes=[
            pltpu.VMEM((8, 8 * W), F32),
            *[pltpu.VMEM((8 * W,), BF16)] * 4,
            pltpu.VMEM((3, 8 * W), BF16),
            pltpu.VMEM((2, 4, ROWS, W), BF16),
            pltpu.VMEM((2, 4, ROWS, W), BF16),
            pltpu.VMEM((ROWS, 8 * W), BF16),
            pltpu.VMEM((4, 512, 3 * W), BF16),
            pltpu.VMEM((4, W, 512), BF16),
            pltpu.VMEM((4, 512, 4 * W), BF16),
            pltpu.VMEM((4, 4 * W, 512), BF16),
            pltpu.VMEM((ROWS, 4 * W), BF16),
            *reduce_scratch,
            *reduce_scratch,
            pltpu.VMEM((ROWS, W), F32),
            pltpu.VMEM((NSEQ, 8, 1, W), F32),
            pltpu.VMEM((ROWS, W), BF16),
            pltpu.SemaphoreType.DMA((NSEND,)),
            pltpu.SemaphoreType.DMA((NRECV,)),
            pltpu.SemaphoreType.DMA((12 + NSEQ,)),
        ],
        compiler_params=pltpu.CompilerParams(
            collective_id=0, has_side_effects=True, vmem_limit_bytes=64 * 1024 * 1024 - 65536
        ),
    )(tokens, bgate_weight, cgate_weight, value_weight, out_weight, up_weight, down_weight,
      mix_in_gain, mix_out_gain, ffn_in_gain, ffn_out_gain, conv_taps)


def solution(mesh):
    torus = Mesh(mesh.devices.reshape(2, 4, 4, 4, 2), ("r", "z", "x", "y", "c"))
    fs, tp = ("z", "x"), ("y", "c")
    return jax.shard_map(
        body,
        mesh=torus,
        in_specs=(
            P(("r", "z", "x"), tp), P(), P(fs, tp), P(fs, tp), P(fs, tp), P(), P(tp, fs),
            P(), P(), P(fs, tp), P(tp, fs), P(),
        ),
        out_specs=P(("r", "z", "x"), tp),
        check_vma=False,
    )
```

```python
import jax
import jax.numpy as jnp
from jax import lax
from jax.experimental import pallas as pl
from jax.experimental.pallas import tpu as pltpu
from jax.sharding import Mesh
from jax.sharding import PartitionSpec as P

EPS = 1e-6
F32 = jnp.float32
BF16 = jnp.bfloat16
LEN = 256
ROWS = 1024
W = 256
NSEQ = ROWS // LEN
NSEND, NRECV = 9, 120
TILE = 64


class Link:
    def __init__(self, send, recv):
        self.send, self.recv, self.sends, self.recvs = send, recv, 0, 0

    def sender(self):
        self.sends += 1
        return self.send.at[self.sends - 1]

    def arrivals(self, n):
        first = self.recvs
        self.recvs += n
        return [self.recv.at[first + k] for k in range(n)]


def copy_of(src, dst, sent, got, device):
    return pltpu.make_async_remote_copy(
        src_ref=src, dst_ref=dst, send_sem=sent, recv_sem=got,
        device_id=device, device_id_type=pl.DeviceIdType.MESH,
    )


class Here:
    def __init__(self):
        r, z, x, y, c = (lax.axis_index(n) for n in ("r", "z", "x", "y", "c"))
        self.z, self.x, self.y, self.c = z, x, y, c
        plus = lambda v, k, n: lax.rem(v + k, n)
        self.xp, self.xo, self.xm = (plus(x, k, 4) for k in (1, 2, 3))
        self.yp, self.yo, self.ym = (plus(y, k, 4) for k in (1, 2, 3))
        self.zp, self.zo, self.zm = (plus(z, k, 4) for k in (1, 2, 3))
        self.cn = 1 - c
        up, down = plus(r * 4 + z, 1, 8), plus(r * 4 + z, 7, 8)
        self.to_xp, self.to_xm = {"x": self.xp}, {"x": self.xm}
        self.to_yp, self.to_ym = {"y": self.yp}, {"y": self.ym}
        self.to_zp = {"r": up // 4, "z": lax.rem(up, 4)}
        self.to_zm = {"r": down // 4, "z": lax.rem(down, 4)}
        self.to_mate = {"c": self.cn}
        self.col = y * 2 + c


def at128(v, n=128):
    return pl.ds(pl.multiple_of(v * 128, 128), n)


class Group:
    def __init__(self, link, here):
        self.h, self.sent = here, link.sender()

    def go(self, src, dst, got, device):
        copy_of(src, dst, self.sent, got, device).start()

    def same(self, mine, got, device):
        self.go(mine, mine, got, device)

    def landed(self, ref, got):
        copy_of(ref, ref, self.sent, got, self.h.to_mate).wait_recv()

    def drain(self, ref):
        copy_of(ref, ref, self.sent, self.sent, self.h.to_mate).wait_send()


class Weight:
    def __init__(self, link, here, buf, by_row):
        self.h, self.buf, self.by_row = here, buf, by_row
        self.half = (buf.shape[2] if by_row else buf.shape[1]) // 2
        self.g = Group(link, here)
        self.r1, self.r2 = link.arrivals(4), link.arrivals(1)[0]
        self.rf, self.rg = link.arrivals(4), link.arrivals(1)[0]

    def unit(self, z, x, part, half=None):
        if self.by_row:
            start, n = (0, 128) if half is None else (64 * half, 64)
            rows = pl.ds(pl.multiple_of(x * 128 + start, 64), n)
            return self.buf.at[z, rows, pl.ds(part * self.half, self.half)]
        q = self.half // 2
        rows = pl.ds(part * self.half, self.half) if half is None else pl.ds(part * self.half + half * q, q)
        return self.buf.at[z, rows, at128(x)]

    def neighbours(self):
        h = self.h
        return (
            ((h.z, h.xm, 0), h.to_xp), ((h.z, h.xp, 0), h.to_xm),
            ((h.zm, h.x, 1), h.to_zp), ((h.zp, h.x, 1), h.to_zm),
        )

    def p1(self, early):
        h = self.h
        for k, (_, dev) in enumerate(self.neighbours()):
            half = k % 2 if early else 1 - k % 2
            self.g.same(self.unit(h.z, h.x, k // 2, half), self.r1[k] if early else self.r2, dev)

    def s1(self):
        for k, (at, dev) in enumerate(self.neighbours()):
            ref = self.unit(*at, k % 2)
            self.g.landed(ref, self.r1[k])
            self.g.same(ref, self.r2, dev)

    def second(self):
        h, u = self.h, self.unit
        a = [lambda z, x=x: u(z, x, 0) for x in (h.x, h.xp, h.xo, h.xm)]
        b = [lambda x, z=z: u(z, x, 1) for z in (h.z, h.zp, h.zo, h.zm)]
        return (
            (a, h.z, h.zm, (0, 1), (2, 3), h.to_zp), (a, h.z, h.zp, (2, 3), (0, 1), h.to_zm),
            (b, h.x, h.xm, (0, 1), (2, 3), h.to_xp), (b, h.x, h.xp, (2, 3), (0, 1), h.to_xm),
        )

    def own2(self):
        for k, (line, here, _, passed, _, dev) in enumerate(self.second()):
            self.g.same(line[0](here), self.rf[k] if 0 in passed else self.rg, dev)

    def s2(self):
        if self.by_row:
            self.g.landed(self.buf.at[0, :, pl.ds(0, self.half)], self.r2)
        else:
            self.g.landed(self.buf.at[0, pl.ds(0, self.half), :], self.r2)
        for first in (True, False):
            for k, (line, here, _, passed, kept, dev) in enumerate(self.second()):
                for n in passed if first else kept:
                    if n:
                        self.g.same(line[n](here), self.rf[k] if first else self.rg, dev)

    def s3(self):
        two = (
            self.buf.at[0, pl.ds(0, 256), pl.ds(0, self.half)] if self.by_row
            else self.buf.at[0, pl.ds(0, self.half), pl.ds(0, 256)]
        )
        for k, (line, _, source, passed, _, dev) in enumerate(self.second()):
            self.g.landed(two, self.rf[k])
            for n in passed:
                self.g.same(line[n](source), self.rg, dev)

    def s4(self):
        self.g.landed(self.buf.at[pl.ds(0, 2)], self.rg)

    def drain(self):
        self.g.drain(self.buf.at[:, pl.ds(0, self.buf.shape[1] // 16 * 15), :])


class Gather:
    def __init__(self, link, group, buf, row, n):
        self.s, self.h, self.buf, self.row, self.n = group, group.h, buf, row, n
        self.f, self.g = link.arrivals(2), link.arrivals(2)
        self.far, self.mate = link.arrivals(2)

    def piece(self, c, y, half=None):
        if half is None:
            return self.buf.at[c, y, pl.ds(self.row, self.n)]
        return self.buf.at[c, y, pl.ds(self.row + half * (self.n // 2), self.n // 2)]

    def t0(self):
        h, s, p = self.h, self.s.same, self.piece
        c, y = h.c, h.y
        s(p(c, y, 0), self.f[0], h.to_yp)
        s(p(c, y, 1), self.f[1], h.to_ym)
        s(p(c, y, 1), self.g[0], h.to_yp)
        s(p(c, y, 0), self.g[1], h.to_ym)
        s(p(c, y), self.mate, h.to_mate)

    def t1(self):
        h, s, p = self.h, self.s.same, self.piece
        c, got = h.c, self.s.landed
        for k, y, dev in ((0, h.ym, h.to_yp), (1, h.yp, h.to_ym)):
            got(p(c, y, k), self.f[k])
            s(p(c, y, k), self.far, dev)

    def t1b(self):
        h, s, p = self.h, self.s.same, self.piece
        c, got = h.c, self.s.landed
        for k, y in ((0, h.ym), (1, h.yp)):
            got(p(c, y, 1 - k), self.g[k])
            s(p(c, y), self.mate, h.to_mate)

    def t2(self):
        h, p = self.h, self.piece
        self.s.landed(p(h.c, h.yo), self.far)
        self.s.same(p(h.c, h.yo), self.mate, h.to_mate)

    def t3(self):
        self.s.landed(self.buf.at[self.h.cn, :, pl.ds(self.row, self.n)], self.mate)


class Reduce:
    def __init__(self, link, group, part, mate, r1, r2, seq):
        self.s, self.h, self.part, self.mate, self.r1, self.r2 = group, group.h, part, mate, r1, r2
        self.seq, self.row = seq, seq * LEN
        self.w0, self.w1, self.w2 = link.arrivals(2), link.arrivals(2), link.arrivals(1)[0]

    def start(self, y, k):
        h, rows = self.h, pl.ds(self.row, LEN)
        self.s.go(self.part.at[h.cn, y, rows], self.mate.at[y, rows], self.w0[k], h.to_mate)

    def both(self, y, lo=0, n=LEN):
        rows = pl.ds(self.row + lo, n)
        return self.part[self.h.c, y, rows, :].astype(F32) + self.mate[y, rows, :].astype(F32)

    def b(self):
        h, half = self.h, LEN // 2
        self.s.landed(self.mate.at[h.yo, pl.ds(self.row, LEN)], self.w0[0])
        for k, dev in ((0, h.to_yp), (1, h.to_ym)):
            rows = pl.ds(self.row + k * half, half)
            self.part[h.c, h.yo, rows, :] = self.both(h.yo, k * half, half).astype(BF16)
            self.s.go(self.part.at[h.c, h.yo, rows], self.r1.at[k, self.seq], self.w1[k], dev)

    def c(self):
        h, half = self.h, LEN // 2
        rows = pl.ds(self.row, LEN)
        self.s.landed(self.mate.at[pl.ds(0, 3), rows], self.w0[1])
        for k, y, dev in ((0, h.yp, h.to_yp), (1, h.ym, h.to_ym)):
            self.s.landed(self.r1.at[k, self.seq], self.w1[k])
            add = self.r1[k, self.seq].astype(F32)
            near, far = self.both(y, k * half, half) + add, self.both(y, (1 - k) * half, half)
            self.part[h.c, y, pl.ds(self.row + k * half, half), :] = near.astype(BF16)
            self.part[h.c, y, pl.ds(self.row + (1 - k) * half, half), :] = far.astype(BF16)
            self.s.go(self.part.at[h.c, y, rows], self.r2.at[k, rows], self.w2, dev)

    def d(self):
        rows = pl.ds(self.row, LEN)
        self.s.landed(self.r2.at[:, rows], self.w2)
        return self.both(self.h.y) + self.r2[0, rows, :].astype(F32) + self.r2[1, rows, :].astype(F32)


def mean_factor(total):
    return lax.rsqrt(total * (1.0 / (8 * W)) + EPS)


def kernel(
    tok, bw, cw, vw, ow, uw, dw, g0, g1, g2, g3, taps3, out,
    consts, ga, gb, gc, gd, taps, X, M, N, WB, WO, WU, WD, ACT, PA, RDA, R1A, R2A, PB, RDB, R1B, R2B, OWN, ST, OUTV,
    send, recv, local,
):
    h = Here()
    link = Link(send, recv)
    early, late, sums, last, stats = (Group(link, h) for _ in range(5))
    own_rows = at128(h.x)
    loads = [
        pltpu.make_async_copy(tok, X.at[h.c, h.y], local.at[0]),
        pltpu.make_async_copy(bw, WB.at[h.z, own_rows, pl.ds(0, W)], local.at[1]),
        pltpu.make_async_copy(cw, WB.at[h.z, own_rows, pl.ds(W, W)], local.at[2]),
        pltpu.make_async_copy(vw, WB.at[h.z, own_rows, pl.ds(2 * W, W)], local.at[3]),
        pltpu.make_async_copy(ow, WO.at[h.z, :, own_rows], local.at[4]),
        pltpu.make_async_copy(uw, WU.at[h.z, own_rows, :], local.at[5]),
        pltpu.make_async_copy(dw, WD.at[h.z, :, own_rows], local.at[6]),
    ] + [
        pltpu.make_async_copy(src, dst, local.at[7 + k])
        for k, (src, dst) in enumerate(((g0, ga), (g1, gb), (g2, gc), (g3, gd), (taps3, taps)))
    ]
    for load in loads:
        load.start()

    peers = [
        {"y": lax.rem(h.y + dy, 4), "c": lax.rem(h.c + dc, 2)}
        for dy in range(4) for dc in range(2) if dy or dc
    ]
    barrier = pltpu.get_barrier_semaphore()
    targets = [h.to_xp, h.to_xm, h.to_zp, h.to_zm] + peers
    for dev in targets:
        pl.semaphore_signal(barrier, inc=1, device_id=dev, device_id_type=pl.DeviceIdType.MESH)
    pl.semaphore_wait(barrier, len(targets))

    toks = [Gather(link, early, X, t * 512, 512) for t in range(2)]
    bcv, outw = Weight(link, h, WB, True), Weight(link, h, WO, False)
    up, down = Weight(link, h, WU, True), Weight(link, h, WD, False)
    mix = [Reduce(link, sums, PA, RDA, R1A, R2A, s) for s in range(NSEQ)]
    ffn = [Reduce(link, last, PB, RDB, R1B, R2B, s) for s in range(NSEQ)]
    mids = [Gather(link, late, M, s * LEN, LEN) for s in range(NSEQ)]

    def total(pieces):
        squares = sum(p * p for p in pieces)
        return jnp.sum(squares, axis=1, keepdims=True)

    def gain(k, j):
        return consts[k : k + 1, j * W : (j + 1) * W]

    def blocks(buf, rows):
        return [buf.at[j % 2, j // 2, rows, :] for j in range(8)]

    def scale_out(source, rows, which):
        factor = mean_factor(total([ref[...].astype(F32) for ref in blocks(source, rows)]))
        for j, ref in enumerate(blocks(source, rows)):
            N[rows, j * W : (j + 1) * W] = (ref[...].astype(F32) * factor * gain(which, j)).astype(BF16)

    def norm_tokens(first, count):
        def tile(i, carry):
            scale_out(X, pl.ds(pl.multiple_of(first + i * TILE, TILE), TILE), 0)
            return carry

        lax.fori_loop(0, count // TILE, tile, 0)

    position = lax.broadcasted_iota(jnp.int32, (LEN, W), 0)
    own_cols = pl.ds(pl.multiple_of(h.col * W, W), W)

    def mixer(s):
        rows = pl.ds(s * LEN, LEN)
        three = jnp.dot(N[rows, :], WB[...].reshape(8 * W, 3 * W), preferred_element_type=F32)
        b, c, v = (three[:, k * W : (k + 1) * W].astype(BF16).astype(F32) for k in range(3))
        inner = c * v
        before = jnp.where(position == 0, 0.0, pltpu.roll(inner, 1, 0))
        after = jnp.where(position == LEN - 1, 0.0, pltpu.roll(inner, LEN - 1, 0))
        tap = [consts[4 + k : 5 + k, own_cols] for k in range(3)]
        conv = tap[0] * before + tap[1] * inner + tap[2] * after
        return (b * conv).astype(BF16)

    def spread(left, weight, part, reduce):
        rows = pl.ds(reduce.row, LEN)

        def block(y):
            piece = jnp.dot(left, weight[y], preferred_element_type=F32).astype(BF16)
            part[0, y, rows, :] = piece[:, :W]
            part[1, y, rows, :] = piece[:, W:]

        block(h.yo)
        reduce.start(h.yo, 0)
        others = (h.yp, h.ym, h.y)
        for y in others:
            block(y)
        for y in others:
            reduce.start(y, 1)

    def A(s, before_out=None):
        gated = mixer(s)
        if before_out:
            before_out()
        spread(gated, WO, PA, mix[s])

    def B(s):
        mix[s].b()

    def C(s):
        mix[s].c()

    def D(s):
        M[h.c, h.y, pl.ds(s * LEN, LEN), :] = mix[s].d().astype(BF16)
        mids[s].t0()

    def Ea(s):
        mids[s].t1()

    def Eb(s):
        mids[s].t1b()

    def F(s):
        mids[s].t2()

    def Ga(s):
        mids[s].t3()

        def tile(i, carry):
            rows = pl.ds(pl.multiple_of(s * LEN + i * TILE, TILE), TILE)
            mixed, kept = blocks(M, rows), blocks(X, rows)
            factor = mean_factor(total([ref[...].astype(F32) for ref in mixed]))
            for j in range(8):
                add = mixed[j][...].astype(F32) * factor * gain(1, j)
                kept[j][...] = (kept[j][...].astype(F32) + add).astype(BF16)
            scale_out(X, rows, 2)
            return carry

        lax.fori_loop(0, LEN // TILE, tile, 0)

    def Gb(s):
        rows = pl.ds(s * LEN, LEN)
        lifted = jnp.dot(N[rows, :], WU[...].reshape(8 * W, 4 * W), preferred_element_type=F32)
        lifted = jnp.maximum(lifted, 0.0)
        ACT[rows, :] = (lifted * lifted).astype(BF16)

    def H(s):
        spread(ACT[pl.ds(s * LEN, LEN), :], WD, PB, ffn[s])

    def D2(s):
        own = ffn[s].d()
        OWN[pl.ds(s * LEN, LEN), :] = own
        energy = jnp.sum((own * own).T, axis=0, keepdims=True)
        ST[s, h.col] = energy
        for dev in peers:
            stats.same(ST.at[s, h.col], known[s], dev)

    def finish(s):
        stats.landed(ST.at[s, pl.ds(0, 7)], known[s])
        factor = mean_factor(sum(ST[s, k] for k in range(8)))
        rows = pl.ds(s * LEN, LEN)
        wide = jnp.broadcast_to(factor, (128, LEN)).T
        wide = jnp.concatenate([wide, wide], axis=1)
        closing = OWN[rows, :] * wide * consts[3:4, own_cols]
        OUTV[rows, :] = (X[h.c, h.y, rows, :].astype(F32) + closing).astype(BF16)
        stored.append(pltpu.make_async_copy(OUTV.at[rows], out.at[rows], local.at[12 + s]))
        stored[-1].start()

    known, stored = link.arrivals(NSEQ), []

    loads[0].wait()
    toks[0].t0()
    toks[1].t0()
    for load in loads[1:4]:
        load.wait()
    bcv.p1(True)
    bcv.p1(False)
    loads[4].wait()
    outw.p1(True)
    outw.p1(False)
    bcv.own2()
    for load in loads[5:]:
        load.wait()
    for k, g in enumerate((ga, gb, gc, gd)):
        consts[k : k + 1, :] = g[...].astype(F32)[None, :]
    consts[4:7, :] = taps[...].astype(F32)

    bcv.s1()
    outw.s1()
    outw.own2()
    up.p1(True)
    bcv.s2()
    outw.s2()
    toks[0].t1()
    toks[0].t1b()
    bcv.s3()
    toks[1].t1()
    toks[1].t1b()
    toks[0].t2()
    toks[0].t3()
    norm_tokens(0, 512)
    outw.s3()
    toks[1].t2()
    toks[1].t3()
    norm_tokens(512, 512)
    bcv.s4()
    up.p1(False)
    up.own2()
    A(0, outw.s4)
    B(0)
    down.p1(True)
    down.p1(False)
    A(1)
    up.s1()
    B(1)
    C(0)
    down.own2()
    A(2)
    B(2)
    C(1)
    up.s2()
    A(3)
    B(3)
    D(0)
    C(2)
    down.s1()
    Ea(0)
    up.s3()
    D(1)
    C(3)
    Eb(0)
    F(0)
    down.s2()
    Ea(1)
    D(2)
    Eb(1)
    early.drain(X.at[:, :, pl.ds(0, 896)])
    Ga(0)
    F(1)
    D(3)
    Ea(2)
    up.s4()
    Gb(0)
    Eb(2)
    down.s3()
    Ga(1)
    Ea(3)
    Gb(1)
    Eb(3)
    F(2)
    F(3)
    Ga(2)
    Gb(2)
    down.s4()
    H(0)
    ffn[0].b()
    H(1)
    ffn[1].b()
    H(2)
    ffn[2].b()
    ffn[0].c()
    Ga(3)
    Gb(3)
    ffn[1].c()
    H(3)
    ffn[3].b()
    ffn[2].c()
    D2(0)
    ffn[3].c()
    D2(1)
    D2(2)
    finish(0)
    D2(3)
    finish(1)
    finish(2)
    finish(3)
    late.drain(M.at[:, :, pl.ds(0, 896)])
    sums.drain(PA.at[:, :, pl.ds(0, 896)])
    last.drain(PB.at[:, :, pl.ds(0, 896)])
    stats.drain(ST.at[:, pl.ds(0, 7)])
    for weight in (bcv, outw, up, down):
        weight.drain()
    for copy in stored:
        copy.wait()


def body(
    tokens, mix_in_gain, bgate_weight, cgate_weight, value_weight, conv_taps, out_weight,
    mix_out_gain, ffn_in_gain, up_weight, down_weight, ffn_out_gain,
):
    hbm = pl.BlockSpec(memory_space=pltpu.HBM)
    reduce_scratch = [
        pltpu.VMEM((2, 4, ROWS, W), BF16),
        pltpu.VMEM((4, ROWS, W), BF16),
        pltpu.VMEM((2, NSEQ, LEN // 2, W), BF16),
        pltpu.VMEM((2, ROWS, W), BF16),
    ]
    return pl.pallas_call(
        kernel,
        out_shape=jax.ShapeDtypeStruct((ROWS, W), BF16),
        in_specs=[hbm] * 12,
        out_specs=hbm,
        scratch_shapes=[
            pltpu.VMEM((8, 8 * W), F32),
            *[pltpu.VMEM((8 * W,), BF16)] * 4,
            pltpu.VMEM((3, 8 * W), BF16),
            pltpu.VMEM((2, 4, ROWS, W), BF16),
            pltpu.VMEM((2, 4, ROWS, W), BF16),
            pltpu.VMEM((ROWS, 8 * W), BF16),
            pltpu.VMEM((4, 512, 3 * W), BF16),
            pltpu.VMEM((4, W, 512), BF16),
            pltpu.VMEM((4, 512, 4 * W), BF16),
            pltpu.VMEM((4, 4 * W, 512), BF16),
            pltpu.VMEM((ROWS, 4 * W), BF16),
            *reduce_scratch,
            *reduce_scratch,
            pltpu.VMEM((ROWS, W), F32),
            pltpu.VMEM((NSEQ, 8, 1, W), F32),
            pltpu.VMEM((ROWS, W), BF16),
            pltpu.SemaphoreType.DMA((NSEND,)),
            pltpu.SemaphoreType.DMA((NRECV,)),
            pltpu.SemaphoreType.DMA((12 + NSEQ,)),
        ],
        compiler_params=pltpu.CompilerParams(
            collective_id=0, has_side_effects=True, vmem_limit_bytes=64 * 1024 * 1024 - 65536
        ),
    )(tokens, bgate_weight, cgate_weight, value_weight, out_weight, up_weight, down_weight,
      mix_in_gain, mix_out_gain, ffn_in_gain, ffn_out_gain, conv_taps)


def solution(mesh):
    torus = Mesh(mesh.devices.reshape(2, 4, 4, 4, 2), ("r", "z", "x", "y", "c"))
    fs, tp = ("z", "x"), ("y", "c")
    return jax.shard_map(
        body,
        mesh=torus,
        in_specs=(
            P(("r", "z", "x"), tp), P(), P(fs, tp), P(fs, tp), P(fs, tp), P(), P(tp, fs),
            P(), P(), P(fs, tp), P(tp, fs), P(),
        ),
        out_specs=P(("r", "z", "x"), tp),
        check_vma=False,
    )
```

```python
import jax
import jax.numpy as jnp
from jax import lax
from jax.experimental import pallas as pl
from jax.experimental.pallas import tpu as pltpu
from jax.sharding import Mesh
from jax.sharding import PartitionSpec as P

EPS = 1e-6
F32 = jnp.float32
BF16 = jnp.bfloat16
LEN = 256
ROWS = 1024
W = 256
NSEQ = ROWS // LEN
NSEND, NRECV = 9, 120
TILE = 64


class Link:
    def __init__(self, send, recv):
        self.send, self.recv, self.sends, self.recvs = send, recv, 0, 0

    def sender(self):
        self.sends += 1
        return self.send.at[self.sends - 1]

    def arrivals(self, n):
        first = self.recvs
        self.recvs += n
        return [self.recv.at[first + k] for k in range(n)]


def copy_of(src, dst, sent, got, device):
    return pltpu.make_async_remote_copy(
        src_ref=src, dst_ref=dst, send_sem=sent, recv_sem=got,
        device_id=device, device_id_type=pl.DeviceIdType.MESH,
    )


class Here:
    def __init__(self):
        r, z, x, y, c = (lax.axis_index(n) for n in ("r", "z", "x", "y", "c"))
        self.z, self.x, self.y, self.c = z, x, y, c
        plus = lambda v, k, n: lax.rem(v + k, n)
        self.xp, self.xo, self.xm = (plus(x, k, 4) for k in (1, 2, 3))
        self.yp, self.yo, self.ym = (plus(y, k, 4) for k in (1, 2, 3))
        self.zp, self.zo, self.zm = (plus(z, k, 4) for k in (1, 2, 3))
        self.cn = 1 - c
        up, down = plus(r * 4 + z, 1, 8), plus(r * 4 + z, 7, 8)
        self.to_xp, self.to_xm = {"x": self.xp}, {"x": self.xm}
        self.to_yp, self.to_ym = {"y": self.yp}, {"y": self.ym}
        self.to_zp = {"r": up // 4, "z": lax.rem(up, 4)}
        self.to_zm = {"r": down // 4, "z": lax.rem(down, 4)}
        self.to_mate = {"c": self.cn}
        self.col = y * 2 + c


def at128(v, n=128):
    return pl.ds(pl.multiple_of(v * 128, 128), n)


class Group:
    def __init__(self, link, here):
        self.h, self.sent = here, link.sender()

    def go(self, src, dst, got, device):
        copy_of(src, dst, self.sent, got, device).start()

    def same(self, mine, got, device):
        self.go(mine, mine, got, device)

    def landed(self, ref, got):
        copy_of(ref, ref, self.sent, got, self.h.to_mate).wait_recv()

    def drain(self, ref):
        copy_of(ref, ref, self.sent, self.sent, self.h.to_mate).wait_send()


class Weight:
    def __init__(self, link, here, buf, by_row):
        self.h, self.buf, self.by_row = here, buf, by_row
        self.half = (buf.shape[2] if by_row else buf.shape[1]) // 2
        self.g = Group(link, here)
        self.r1, self.r2 = link.arrivals(4), link.arrivals(1)[0]
        self.rf, self.rg = link.arrivals(4), link.arrivals(1)[0]

    def unit(self, z, x, part, half=None):
        if self.by_row:
            start, n = (0, 128) if half is None else (64 * half, 64)
            rows = pl.ds(pl.multiple_of(x * 128 + start, 64), n)
            return self.buf.at[z, rows, pl.ds(part * self.half, self.half)]
        q = self.half // 2
        rows = pl.ds(part * self.half, self.half) if half is None else pl.ds(part * self.half + half * q, q)
        return self.buf.at[z, rows, at128(x)]

    def neighbours(self):
        h = self.h
        return (
            ((h.z, h.xm, 0), h.to_xp), ((h.z, h.xp, 0), h.to_xm),
            ((h.zm, h.x, 1), h.to_zp), ((h.zp, h.x, 1), h.to_zm),
        )

    def p1(self, early):
        h = self.h
        for k, (_, dev) in enumerate(self.neighbours()):
            half = k % 2 if early else 1 - k % 2
            self.g.same(self.unit(h.z, h.x, k // 2, half), self.r1[k] if early else self.r2, dev)

    def s1(self):
        for k, (at, dev) in enumerate(self.neighbours()):
            ref = self.unit(*at, k % 2)
            self.g.landed(ref, self.r1[k])
            self.g.same(ref, self.r2, dev)

    def second(self):
        h, u = self.h, self.unit
        a = [lambda z, x=x: u(z, x, 0) for x in (h.x, h.xp, h.xo, h.xm)]
        b = [lambda x, z=z: u(z, x, 1) for z in (h.z, h.zp, h.zo, h.zm)]
        return (
            (a, h.z, h.zm, (0, 1), (2, 3), h.to_zp), (a, h.z, h.zp, (2, 3), (0, 1), h.to_zm),
            (b, h.x, h.xm, (0, 1), (2, 3), h.to_xp), (b, h.x, h.xp, (2, 3), (0, 1), h.to_xm),
        )

    def own2(self):
        for k, (line, here, _, passed, _, dev) in enumerate(self.second()):
            self.g.same(line[0](here), self.rf[k] if 0 in passed else self.rg, dev)

    def s2(self):
        if self.by_row:
            self.g.landed(self.buf.at[0, :, pl.ds(0, self.half)], self.r2)
        else:
            self.g.landed(self.buf.at[0, pl.ds(0, self.half), :], self.r2)
        for first in (True, False):
            for k, (line, here, _, passed, kept, dev) in enumerate(self.second()):
                for n in passed if first else kept:
                    if n:
                        self.g.same(line[n](here), self.rf[k] if first else self.rg, dev)

    def s3(self):
        two = (
            self.buf.at[0, pl.ds(0, 256), pl.ds(0, self.half)] if self.by_row
            else self.buf.at[0, pl.ds(0, self.half), pl.ds(0, 256)]
        )
        for k, (line, _, source, passed, _, dev) in enumerate(self.second()):
            self.g.landed(two, self.rf[k])
            for n in passed:
                self.g.same(line[n](source), self.rg, dev)

    def s4(self):
        self.g.landed(self.buf.at[pl.ds(0, 2)], self.rg)

    def drain(self):
        self.g.drain(self.buf.at[:, pl.ds(0, self.buf.shape[1] // 16 * 15), :])


class Gather:
    def __init__(self, link, group, buf, row, n):
        self.s, self.h, self.buf, self.row, self.n = group, group.h, buf, row, n
        self.f, self.g = link.arrivals(2), link.arrivals(2)
        self.far, self.mate = link.arrivals(2)

    def piece(self, c, y, half=None):
        if half is None:
            return self.buf.at[c, y, pl.ds(self.row, self.n)]
        return self.buf.at[c, y, pl.ds(self.row + half * (self.n // 2), self.n // 2)]

    def t0(self):
        h, s, p = self.h, self.s.same, self.piece
        c, y = h.c, h.y
        s(p(c, y, 0), self.f[0], h.to_yp)
        s(p(c, y, 1), self.f[1], h.to_ym)
        s(p(c, y, 1), self.g[0], h.to_yp)
        s(p(c, y, 0), self.g[1], h.to_ym)
        s(p(c, y), self.mate, h.to_mate)

    def t1(self):
        h, s, p = self.h, self.s.same, self.piece
        c, got = h.c, self.s.landed
        for k, y, dev in ((0, h.ym, h.to_yp), (1, h.yp, h.to_ym)):
            got(p(c, y, k), self.f[k])
            s(p(c, y, k), self.far, dev)

    def t1b(self):
        h, s, p = self.h, self.s.same, self.piece
        c, got = h.c, self.s.landed
        for k, y in ((0, h.ym), (1, h.yp)):
            got(p(c, y, 1 - k), self.g[k])
            s(p(c, y), self.mate, h.to_mate)

    def t2(self):
        h, p = self.h, self.piece
        self.s.landed(p(h.c, h.yo), self.far)
        self.s.same(p(h.c, h.yo), self.mate, h.to_mate)

    def t3(self):
        self.s.landed(self.buf.at[self.h.cn, :, pl.ds(self.row, self.n)], self.mate)


class Reduce:
    def __init__(self, link, group, part, mate, r1, r2, seq):
        self.s, self.h, self.part, self.mate, self.r1, self.r2 = group, group.h, part, mate, r1, r2
        self.seq, self.row = seq, seq * LEN
        self.w0, self.w1, self.w2 = link.arrivals(2), link.arrivals(2), link.arrivals(1)[0]

    def start(self, y, k):
        h, rows = self.h, pl.ds(self.row, LEN)
        self.s.go(self.part.at[h.cn, y, rows], self.mate.at[y, rows], self.w0[k], h.to_mate)

    def both(self, y, lo=0, n=LEN):
        rows = pl.ds(self.row + lo, n)
        return self.part[self.h.c, y, rows, :].astype(F32) + self.mate[y, rows, :].astype(F32)

    def b(self):
        h, half = self.h, LEN // 2
        self.s.landed(self.mate.at[h.yo, pl.ds(self.row, LEN)], self.w0[0])
        for k, dev in ((0, h.to_yp), (1, h.to_ym)):
            rows = pl.ds(self.row + k * half, half)
            self.part[h.c, h.yo, rows, :] = self.both(h.yo, k * half, half).astype(BF16)
            self.s.go(self.part.at[h.c, h.yo, rows], self.r1.at[k, self.seq], self.w1[k], dev)

    def c(self):
        h, half = self.h, LEN // 2
        rows = pl.ds(self.row, LEN)
        self.s.landed(self.mate.at[pl.ds(0, 3), rows], self.w0[1])
        for k, y, dev in ((0, h.yp, h.to_yp), (1, h.ym, h.to_ym)):
            self.s.landed(self.r1.at[k, self.seq], self.w1[k])
            add = self.r1[k, self.seq].astype(F32)
            near, far = self.both(y, k * half, half) + add, self.both(y, (1 - k) * half, half)
            self.part[h.c, y, pl.ds(self.row + k * half, half), :] = near.astype(BF16)
            self.part[h.c, y, pl.ds(self.row + (1 - k) * half, half), :] = far.astype(BF16)
            self.s.go(self.part.at[h.c, y, rows], self.r2.at[k, rows], self.w2, dev)

    def d(self):
        rows = pl.ds(self.row, LEN)
        self.s.landed(self.r2.at[:, rows], self.w2)
        return self.both(self.h.y) + self.r2[0, rows, :].astype(F32) + self.r2[1, rows, :].astype(F32)


def mean_factor(total):
    return lax.rsqrt(total * (1.0 / (8 * W)) + EPS)


def kernel(
    tok, bw, cw, vw, ow, uw, dw, g0, g1, g2, g3, taps3, out,
    consts, ga, gb, gc, gd, taps, X, M, N, WB, WO, WU, WD, ACT, PA, RDA, R1A, R2A, PB, RDB, R1B, R2B, OWN, ST, OUTV,
    send, recv, local,
):
    h = Here()
    link = Link(send, recv)
    early, late, sums, last, stats = (Group(link, h) for _ in range(5))
    own_rows = at128(h.x)
    loads = [
        pltpu.make_async_copy(tok, X.at[h.c, h.y], local.at[0]),
        pltpu.make_async_copy(bw, WB.at[h.z, own_rows, pl.ds(0, W)], local.at[1]),
        pltpu.make_async_copy(cw, WB.at[h.z, own_rows, pl.ds(W, W)], local.at[2]),
        pltpu.make_async_copy(vw, WB.at[h.z, own_rows, pl.ds(2 * W, W)], local.at[3]),
        pltpu.make_async_copy(ow, WO.at[h.z, :, own_rows], local.at[4]),
        pltpu.make_async_copy(uw, WU.at[h.z, own_rows, :], local.at[5]),
        pltpu.make_async_copy(dw, WD.at[h.z, :, own_rows], local.at[6]),
    ] + [
        pltpu.make_async_copy(src, dst, local.at[7 + k])
        for k, (src, dst) in enumerate(((g0, ga), (g1, gb), (g2, gc), (g3, gd), (taps3, taps)))
    ]
    for load in loads:
        load.start()

    peers = [
        {"y": lax.rem(h.y + dy, 4), "c": lax.rem(h.c + dc, 2)}
        for dy in range(4) for dc in range(2) if dy or dc
    ]
    barrier = pltpu.get_barrier_semaphore()
    targets = [h.to_xp, h.to_xm, h.to_zp, h.to_zm] + peers
    for dev in targets:
        pl.semaphore_signal(barrier, inc=1, device_id=dev, device_id_type=pl.DeviceIdType.MESH)
    pl.semaphore_wait(barrier, len(targets))

    toks = [Gather(link, early, X, t * 512, 512) for t in range(2)]
    bcv, outw = Weight(link, h, WB, True), Weight(link, h, WO, False)
    up, down = Weight(link, h, WU, True), Weight(link, h, WD, False)
    mix = [Reduce(link, sums, PA, RDA, R1A, R2A, s) for s in range(NSEQ)]
    ffn = [Reduce(link, last, PB, RDB, R1B, R2B, s) for s in range(NSEQ)]
    mids = [Gather(link, late, M, s * LEN, LEN) for s in range(NSEQ)]

    def total(pieces):
        squares = sum(p * p for p in pieces)
        return jnp.sum(squares, axis=1, keepdims=True)

    def gain(k, j):
        return consts[k : k + 1, j * W : (j + 1) * W]

    def blocks(buf, rows):
        return [buf.at[j % 2, j // 2, rows, :] for j in range(8)]

    def scale_out(source, rows, which):
        factor = mean_factor(total([ref[...].astype(F32) for ref in blocks(source, rows)]))
        for j, ref in enumerate(blocks(source, rows)):
            N[rows, j * W : (j + 1) * W] = (ref[...].astype(F32) * factor * gain(which, j)).astype(BF16)

    def norm_tokens(first, count):
        def tile(i, carry):
            scale_out(X, pl.ds(pl.multiple_of(first + i * TILE, TILE), TILE), 0)
            return carry

        lax.fori_loop(0, count // TILE, tile, 0)

    position = lax.broadcasted_iota(jnp.int32, (LEN, W), 0)
    own_cols = pl.ds(pl.multiple_of(h.col * W, W), W)

    def mixer(s):
        rows = pl.ds(s * LEN, LEN)
        three = jnp.dot(N[rows, :], WB[...].reshape(8 * W, 3 * W), preferred_element_type=F32)
        b, c, v = (three[:, k * W : (k + 1) * W].astype(BF16).astype(F32) for k in range(3))
        inner = c * v
        before = jnp.where(position == 0, 0.0, pltpu.roll(inner, 1, 0))
        after = jnp.where(position == LEN - 1, 0.0, pltpu.roll(inner, LEN - 1, 0))
        tap = [consts[4 + k : 5 + k, own_cols] for k in range(3)]
        conv = tap[0] * before + tap[1] * inner + tap[2] * after
        return (b * conv).astype(BF16)

    def spread(left, weight, part, reduce):
        rows = pl.ds(reduce.row, LEN)

        def block(y):
            piece = jnp.dot(left, weight[y], preferred_element_type=F32).astype(BF16)
            part[0, y, rows, :] = piece[:, :W]
            part[1, y, rows, :] = piece[:, W:]

        block(h.yo)
        reduce.start(h.yo, 0)
        others = (h.yp, h.ym, h.y)
        for y in others:
            block(y)
        for y in others:
            reduce.start(y, 1)

    def A(s, before_out=None):
        gated = mixer(s)
        if before_out:
            before_out()
        spread(gated, WO, PA, mix[s])

    def B(s):
        mix[s].b()

    def C(s):
        mix[s].c()

    def D(s):
        M[h.c, h.y, pl.ds(s * LEN, LEN), :] = mix[s].d().astype(BF16)
        mids[s].t0()

    def Ea(s):
        mids[s].t1()

    def Eb(s):
        mids[s].t1b()

    def F(s):
        mids[s].t2()

    def Ga(s):
        mids[s].t3()

        def tile(i, carry):
            rows = pl.ds(pl.multiple_of(s * LEN + i * TILE, TILE), TILE)
            mixed, kept = blocks(M, rows), blocks(X, rows)
            factor = mean_factor(total([ref[...].astype(F32) for ref in mixed]))
            for j in range(8):
                add = mixed[j][...].astype(F32) * factor * gain(1, j)
                kept[j][...] = (kept[j][...].astype(F32) + add).astype(BF16)
            scale_out(X, rows, 2)
            return carry

        lax.fori_loop(0, LEN // TILE, tile, 0)

    def Gb(s):
        rows = pl.ds(s * LEN, LEN)
        lifted = jnp.dot(N[rows, :], WU[...].reshape(8 * W, 4 * W), preferred_element_type=F32)
        lifted = jnp.maximum(lifted, 0.0)
        ACT[rows, :] = (lifted * lifted).astype(BF16)

    def H(s):
        spread(ACT[pl.ds(s * LEN, LEN), :], WD, PB, ffn[s])

    def D2(s):
        own = ffn[s].d()
        OWN[pl.ds(s * LEN, LEN), :] = own
        energy = jnp.sum((own * own).T, axis=0, keepdims=True)
        ST[s, h.col] = energy
        for dev in peers:
            stats.same(ST.at[s, h.col], known[s], dev)

    def finish(s):
        stats.landed(ST.at[s, pl.ds(0, 7)], known[s])
        factor = mean_factor(sum(ST[s, k] for k in range(8)))
        rows = pl.ds(s * LEN, LEN)
        wide = jnp.broadcast_to(factor, (128, LEN)).T
        wide = jnp.concatenate([wide, wide], axis=1)
        closing = OWN[rows, :] * wide * consts[3:4, own_cols]
        OUTV[rows, :] = (X[h.c, h.y, rows, :].astype(F32) + closing).astype(BF16)
        stored.append(pltpu.make_async_copy(OUTV.at[rows], out.at[rows], local.at[12 + s]))
        stored[-1].start()

    known, stored = link.arrivals(NSEQ), []

    loads[0].wait()
    toks[0].t0()
    toks[1].t0()
    for load in loads[1:4]:
        load.wait()
    bcv.p1(True)
    bcv.p1(False)
    loads[4].wait()
    outw.p1(True)
    outw.p1(False)
    bcv.own2()
    for load in loads[5:]:
        load.wait()
    for k, g in enumerate((ga, gb, gc, gd)):
        consts[k : k + 1, :] = g[...].astype(F32)[None, :]
    consts[4:7, :] = taps[...].astype(F32)

    bcv.s1()
    outw.s1()
    outw.own2()
    up.p1(True)
    bcv.s2()
    outw.s2()
    toks[0].t1()
    toks[0].t1b()
    bcv.s3()
    toks[1].t1()
    toks[1].t1b()
    toks[0].t2()
    toks[0].t3()
    norm_tokens(0, 512)
    outw.s3()
    toks[1].t2()
    toks[1].t3()
    norm_tokens(512, 512)
    bcv.s4()
    up.s1()
    up.p1(False)
    up.own2()
    A(0, outw.s4)
    B(0)
    down.p1(True)
    down.p1(False)
    A(1)
    up.s2()
    B(1)
    C(0)
    A(2)
    B(2)
    C(1)
    down.s1()
    down.own2()
    A(3)
    B(3)
    D(0)
    C(2)
    up.s3()
    Ea(0)
    D(1)
    C(3)
    down.s2()
    Eb(0)
    F(0)
    Ea(1)
    D(2)
    Eb(1)
    early.drain(X.at[:, :, pl.ds(0, 896)])
    Ga(0)
    F(1)
    D(3)
    down.s3()
    Ea(2)
    up.s4()
    Gb(0)
    Eb(2)
    Ga(1)
    Ea(3)
    Gb(1)
    Eb(3)
    F(2)
    F(3)
    Ga(2)
    Gb(2)
    down.s4()
    H(0)
    ffn[0].b()
    H(1)
    ffn[1].b()
    H(2)
    ffn[2].b()
    ffn[0].c()
    Ga(3)
    Gb(3)
    ffn[1].c()
    H(3)
    ffn[3].b()
    ffn[2].c()
    D2(0)
    ffn[3].c()
    D2(1)
    D2(2)
    finish(0)
    D2(3)
    finish(1)
    finish(2)
    finish(3)
    late.drain(M.at[:, :, pl.ds(0, 896)])
    sums.drain(PA.at[:, :, pl.ds(0, 896)])
    last.drain(PB.at[:, :, pl.ds(0, 896)])
    stats.drain(ST.at[:, pl.ds(0, 7)])
    for weight in (bcv, outw, up, down):
        weight.drain()
    for copy in stored:
        copy.wait()


def body(
    tokens, mix_in_gain, bgate_weight, cgate_weight, value_weight, conv_taps, out_weight,
    mix_out_gain, ffn_in_gain, up_weight, down_weight, ffn_out_gain,
):
    hbm = pl.BlockSpec(memory_space=pltpu.HBM)
    reduce_scratch = [
        pltpu.VMEM((2, 4, ROWS, W), BF16),
        pltpu.VMEM((4, ROWS, W), BF16),
        pltpu.VMEM((2, NSEQ, LEN // 2, W), BF16),
        pltpu.VMEM((2, ROWS, W), BF16),
    ]
    return pl.pallas_call(
        kernel,
        out_shape=jax.ShapeDtypeStruct((ROWS, W), BF16),
        in_specs=[hbm] * 12,
        out_specs=hbm,
        scratch_shapes=[
            pltpu.VMEM((8, 8 * W), F32),
            *[pltpu.VMEM((8 * W,), BF16)] * 4,
            pltpu.VMEM((3, 8 * W), BF16),
            pltpu.VMEM((2, 4, ROWS, W), BF16),
            pltpu.VMEM((2, 4, ROWS, W), BF16),
            pltpu.VMEM((ROWS, 8 * W), BF16),
            pltpu.VMEM((4, 512, 3 * W), BF16),
            pltpu.VMEM((4, W, 512), BF16),
            pltpu.VMEM((4, 512, 4 * W), BF16),
            pltpu.VMEM((4, 4 * W, 512), BF16),
            pltpu.VMEM((ROWS, 4 * W), BF16),
            *reduce_scratch,
            *reduce_scratch,
            pltpu.VMEM((ROWS, W), F32),
            pltpu.VMEM((NSEQ, 8, 1, W), F32),
            pltpu.VMEM((ROWS, W), BF16),
            pltpu.SemaphoreType.DMA((NSEND,)),
            pltpu.SemaphoreType.DMA((NRECV,)),
            pltpu.SemaphoreType.DMA((12 + NSEQ,)),
        ],
        compiler_params=pltpu.CompilerParams(
            collective_id=0, has_side_effects=True, vmem_limit_bytes=64 * 1024 * 1024 - 65536
        ),
    )(tokens, bgate_weight, cgate_weight, value_weight, out_weight, up_weight, down_weight,
      mix_in_gain, mix_out_gain, ffn_in_gain, ffn_out_gain, conv_taps)


def solution(mesh):
    torus = Mesh(mesh.devices.reshape(2, 4, 4, 4, 2), ("r", "z", "x", "y", "c"))
    fs, tp = ("z", "x"), ("y", "c")
    return jax.shard_map(
        body,
        mesh=torus,
        in_specs=(
            P(("r", "z", "x"), tp), P(), P(fs, tp), P(fs, tp), P(fs, tp), P(), P(tp, fs),
            P(), P(), P(fs, tp), P(tp, fs), P(),
        ),
        out_specs=P(("r", "z", "x"), tp),
        check_vma=False,
    )
```

```python
import jax
import jax.numpy as jnp
from jax import lax
from jax.experimental import pallas as pl
from jax.experimental.pallas import tpu as pltpu
from jax.sharding import Mesh
from jax.sharding import PartitionSpec as P

EPS = 1e-6
F32 = jnp.float32
BF16 = jnp.bfloat16
LEN = 256
ROWS = 1024
W = 256
NSEQ = ROWS // LEN
NSEND, NRECV = 9, 120
TILE = 64


class Link:
    def __init__(self, send, recv):
        self.send, self.recv, self.sends, self.recvs = send, recv, 0, 0

    def sender(self):
        self.sends += 1
        return self.send.at[self.sends - 1]

    def arrivals(self, n):
        first = self.recvs
        self.recvs += n
        return [self.recv.at[first + k] for k in range(n)]


def copy_of(src, dst, sent, got, device):
    return pltpu.make_async_remote_copy(
        src_ref=src, dst_ref=dst, send_sem=sent, recv_sem=got,
        device_id=device, device_id_type=pl.DeviceIdType.MESH,
    )


class Here:
    def __init__(self):
        r, z, x, y, c = (lax.axis_index(n) for n in ("r", "z", "x", "y", "c"))
        self.z, self.x, self.y, self.c = z, x, y, c
        plus = lambda v, k, n: lax.rem(v + k, n)
        self.xp, self.xo, self.xm = (plus(x, k, 4) for k in (1, 2, 3))
        self.yp, self.yo, self.ym = (plus(y, k, 4) for k in (1, 2, 3))
        self.zp, self.zo, self.zm = (plus(z, k, 4) for k in (1, 2, 3))
        self.cn = 1 - c
        up, down = plus(r * 4 + z, 1, 8), plus(r * 4 + z, 7, 8)
        self.to_xp, self.to_xm = {"x": self.xp}, {"x": self.xm}
        self.to_yp, self.to_ym = {"y": self.yp}, {"y": self.ym}
        self.to_zp = {"r": up // 4, "z": lax.rem(up, 4)}
        self.to_zm = {"r": down // 4, "z": lax.rem(down, 4)}
        self.to_mate = {"c": self.cn}
        self.col = y * 2 + c


def at128(v, n=128):
    return pl.ds(pl.multiple_of(v * 128, 128), n)


class Group:
    def __init__(self, link, here):
        self.h, self.sent = here, link.sender()

    def go(self, src, dst, got, device):
        copy_of(src, dst, self.sent, got, device).start()

    def same(self, mine, got, device):
        self.go(mine, mine, got, device)

    def landed(self, ref, got):
        copy_of(ref, ref, self.sent, got, self.h.to_mate).wait_recv()

    def drain(self, ref):
        copy_of(ref, ref, self.sent, self.sent, self.h.to_mate).wait_send()


class Weight:
    def __init__(self, link, here, buf, by_row):
        self.h, self.buf, self.by_row = here, buf, by_row
        self.half = (buf.shape[2] if by_row else buf.shape[1]) // 2
        self.g = Group(link, here)
        self.r1, self.r2 = link.arrivals(4), link.arrivals(1)[0]
        self.rf, self.rg = link.arrivals(4), link.arrivals(1)[0]

    def unit(self, z, x, part, half=None):
        if self.by_row:
            start, n = (0, 128) if half is None else (64 * half, 64)
            rows = pl.ds(pl.multiple_of(x * 128 + start, 64), n)
            return self.buf.at[z, rows, pl.ds(part * self.half, self.half)]
        q = self.half // 2
        rows = pl.ds(part * self.half, self.half) if half is None else pl.ds(part * self.half + half * q, q)
        return self.buf.at[z, rows, at128(x)]

    def neighbours(self):
        h = self.h
        return (
            ((h.z, h.xm, 0), h.to_xp), ((h.z, h.xp, 0), h.to_xm),
            ((h.zm, h.x, 1), h.to_zp), ((h.zp, h.x, 1), h.to_zm),
        )

    def p1(self, early):
        h = self.h
        for k, (_, dev) in enumerate(self.neighbours()):
            half = k % 2 if early else 1 - k % 2
            self.g.same(self.unit(h.z, h.x, k // 2, half), self.r1[k] if early else self.r2, dev)

    def s1(self):
        for k, (at, dev) in enumerate(self.neighbours()):
            ref = self.unit(*at, k % 2)
            self.g.landed(ref, self.r1[k])
            self.g.same(ref, self.r2, dev)

    def second(self):
        h, u = self.h, self.unit
        a = [lambda z, x=x: u(z, x, 0) for x in (h.x, h.xp, h.xo, h.xm)]
        b = [lambda x, z=z: u(z, x, 1) for z in (h.z, h.zp, h.zo, h.zm)]
        return (
            (a, h.z, h.zm, (0, 1), (2, 3), h.to_zp), (a, h.z, h.zp, (2, 3), (0, 1), h.to_zm),
            (b, h.x, h.xm, (0, 1), (2, 3), h.to_xp), (b, h.x, h.xp, (2, 3), (0, 1), h.to_xm),
        )

    def own2(self):
        for k, (line, here, _, passed, _, dev) in enumerate(self.second()):
            self.g.same(line[0](here), self.rf[k] if 0 in passed else self.rg, dev)

    def s2(self):
        if self.by_row:
            self.g.landed(self.buf.at[0, :, pl.ds(0, self.half)], self.r2)
        else:
            self.g.landed(self.buf.at[0, pl.ds(0, self.half), :], self.r2)
        for first in (True, False):
            for k, (line, here, _, passed, kept, dev) in enumerate(self.second()):
                for n in passed if first else kept:
                    if n:
                        self.g.same(line[n](here), self.rf[k] if first else self.rg, dev)

    def s3(self):
        two = (
            self.buf.at[0, pl.ds(0, 256), pl.ds(0, self.half)] if self.by_row
            else self.buf.at[0, pl.ds(0, self.half), pl.ds(0, 256)]
        )
        for k, (line, _, source, passed, _, dev) in enumerate(self.second()):
            self.g.landed(two, self.rf[k])
            for n in passed:
                self.g.same(line[n](source), self.rg, dev)

    def s4(self):
        self.g.landed(self.buf.at[pl.ds(0, 2)], self.rg)

    def drain(self):
        self.g.drain(self.buf.at[:, pl.ds(0, self.buf.shape[1] // 16 * 15), :])


class Gather:
    def __init__(self, link, group, buf, row, n):
        self.s, self.h, self.buf, self.row, self.n = group, group.h, buf, row, n
        self.f, self.g = link.arrivals(2), link.arrivals(2)
        self.far, self.mate = link.arrivals(2)

    def piece(self, c, y, half=None):
        if half is None:
            return self.buf.at[c, y, pl.ds(self.row, self.n)]
        return self.buf.at[c, y, pl.ds(self.row + half * (self.n // 2), self.n // 2)]

    def t0(self):
        h, s, p = self.h, self.s.same, self.piece
        c, y = h.c, h.y
        s(p(c, y, 0), self.f[0], h.to_yp)
        s(p(c, y, 1), self.f[1], h.to_ym)
        s(p(c, y, 1), self.g[0], h.to_yp)
        s(p(c, y, 0), self.g[1], h.to_ym)
        s(p(c, y), self.mate, h.to_mate)

    def t1(self):
        h, s, p = self.h, self.s.same, self.piece
        c, got = h.c, self.s.landed
        for k, y, dev in ((0, h.ym, h.to_yp), (1, h.yp, h.to_ym)):
            got(p(c, y, k), self.f[k])
            s(p(c, y, k), self.far, dev)

    def t1b(self):
        h, s, p = self.h, self.s.same, self.piece
        c, got = h.c, self.s.landed
        for k, y in ((0, h.ym), (1, h.yp)):
            got(p(c, y, 1 - k), self.g[k])
            s(p(c, y), self.mate, h.to_mate)

    def t2(self):
        h, p = self.h, self.piece
        self.s.landed(p(h.c, h.yo), self.far)
        self.s.same(p(h.c, h.yo), self.mate, h.to_mate)

    def t3(self):
        self.s.landed(self.buf.at[self.h.cn, :, pl.ds(self.row, self.n)], self.mate)


class Reduce:
    def __init__(self, link, group, part, mate, r1, r2, seq):
        self.s, self.h, self.part, self.mate, self.r1, self.r2 = group, group.h, part, mate, r1, r2
        self.seq, self.row = seq, seq * LEN
        self.w0, self.w1, self.w2 = link.arrivals(2), link.arrivals(2), link.arrivals(1)[0]

    def start(self, y, k):
        h, rows = self.h, pl.ds(self.row, LEN)
        self.s.go(self.part.at[h.cn, y, rows], self.mate.at[y, rows], self.w0[k], h.to_mate)

    def both(self, y, lo=0, n=LEN):
        rows = pl.ds(self.row + lo, n)
        return self.part[self.h.c, y, rows, :].astype(F32) + self.mate[y, rows, :].astype(F32)

    def b(self):
        h, half = self.h, LEN // 2
        self.s.landed(self.mate.at[h.yo, pl.ds(self.row, LEN)], self.w0[0])
        for k, dev in ((0, h.to_yp), (1, h.to_ym)):
            rows = pl.ds(self.row + k * half, half)
            self.part[h.c, h.yo, rows, :] = self.both(h.yo, k * half, half).astype(BF16)
            self.s.go(self.part.at[h.c, h.yo, rows], self.r1.at[k, self.seq], self.w1[k], dev)

    def c(self):
        h, half = self.h, LEN // 2
        rows = pl.ds(self.row, LEN)
        self.s.landed(self.mate.at[pl.ds(0, 3), rows], self.w0[1])
        for k, y, dev in ((0, h.yp, h.to_yp), (1, h.ym, h.to_ym)):
            self.s.landed(self.r1.at[k, self.seq], self.w1[k])
            add = self.r1[k, self.seq].astype(F32)
            near, far = self.both(y, k * half, half) + add, self.both(y, (1 - k) * half, half)
            self.part[h.c, y, pl.ds(self.row + k * half, half), :] = near.astype(BF16)
            self.part[h.c, y, pl.ds(self.row + (1 - k) * half, half), :] = far.astype(BF16)
            self.s.go(self.part.at[h.c, y, rows], self.r2.at[k, rows], self.w2, dev)

    def d(self):
        rows = pl.ds(self.row, LEN)
        self.s.landed(self.r2.at[:, rows], self.w2)
        return self.both(self.h.y) + self.r2[0, rows, :].astype(F32) + self.r2[1, rows, :].astype(F32)


def mean_factor(total):
    return lax.rsqrt(total * (1.0 / (8 * W)) + EPS)


def kernel(
    tok, bw, cw, vw, ow, uw, dw, g0, g1, g2, g3, taps3, out,
    consts, ga, gb, gc, gd, taps, X, M, N, WB, WO, WU, WD, ACT, PA, RDA, R1A, R2A, PB, RDB, R1B, R2B, OWN, ST, OUTV,
    send, recv, local,
):
    h = Here()
    link = Link(send, recv)
    early, late, sums, last, stats = (Group(link, h) for _ in range(5))
    own_rows = at128(h.x)
    loads = [
        pltpu.make_async_copy(tok, X.at[h.c, h.y], local.at[0]),
        pltpu.make_async_copy(bw, WB.at[h.z, own_rows, pl.ds(0, W)], local.at[1]),
        pltpu.make_async_copy(cw, WB.at[h.z, own_rows, pl.ds(W, W)], local.at[2]),
        pltpu.make_async_copy(vw, WB.at[h.z, own_rows, pl.ds(2 * W, W)], local.at[3]),
        pltpu.make_async_copy(ow, WO.at[h.z, :, own_rows], local.at[4]),
        pltpu.make_async_copy(uw, WU.at[h.z, own_rows, :], local.at[5]),
        pltpu.make_async_copy(dw, WD.at[h.z, :, own_rows], local.at[6]),
    ] + [
        pltpu.make_async_copy(src, dst, local.at[7 + k])
        for k, (src, dst) in enumerate(((g0, ga), (g1, gb), (g2, gc), (g3, gd), (taps3, taps)))
    ]
    for load in loads:
        load.start()

    peers = [
        {"y": lax.rem(h.y + dy, 4), "c": lax.rem(h.c + dc, 2)}
        for dy in range(4) for dc in range(2) if dy or dc
    ]
    barrier = pltpu.get_barrier_semaphore()
    targets = [h.to_xp, h.to_xm, h.to_zp, h.to_zm] + peers
    for dev in targets:
        pl.semaphore_signal(barrier, inc=1, device_id=dev, device_id_type=pl.DeviceIdType.MESH)
    pl.semaphore_wait(barrier, len(targets))

    toks = [Gather(link, early, X, t * 512, 512) for t in range(2)]
    bcv, outw = Weight(link, h, WB, True), Weight(link, h, WO, False)
    up, down = Weight(link, h, WU, True), Weight(link, h, WD, False)
    mix = [Reduce(link, sums, PA, RDA, R1A, R2A, s) for s in range(NSEQ)]
    ffn = [Reduce(link, last, PB, RDB, R1B, R2B, s) for s in range(NSEQ)]
    mids = [Gather(link, late, M, s * LEN, LEN) for s in range(NSEQ)]

    def total(pieces):
        squares = sum(p * p for p in pieces)
        return jnp.sum(squares, axis=1, keepdims=True)

    def gain(k, j):
        return consts[k : k + 1, j * W : (j + 1) * W]

    def blocks(buf, rows):
        return [buf.at[j % 2, j // 2, rows, :] for j in range(8)]

    def scale_out(source, rows, which):
        factor = mean_factor(total([ref[...].astype(F32) for ref in blocks(source, rows)]))
        for j, ref in enumerate(blocks(source, rows)):
            N[rows, j * W : (j + 1) * W] = (ref[...].astype(F32) * factor * gain(which, j)).astype(BF16)

    def norm_tokens(first, count):
        def tile(i, carry):
            scale_out(X, pl.ds(pl.multiple_of(first + i * TILE, TILE), TILE), 0)
            return carry

        lax.fori_loop(0, count // TILE, tile, 0)

    position = lax.broadcasted_iota(jnp.int32, (LEN, W), 0)
    own_cols = pl.ds(pl.multiple_of(h.col * W, W), W)

    def mixer(s):
        rows = pl.ds(s * LEN, LEN)
        three = jnp.dot(N[rows, :], WB[...].reshape(8 * W, 3 * W), preferred_element_type=F32)
        b, c, v = (three[:, k * W : (k + 1) * W].astype(BF16).astype(F32) for k in range(3))
        inner = c * v
        before = jnp.where(position == 0, 0.0, pltpu.roll(inner, 1, 0))
        after = jnp.where(position == LEN - 1, 0.0, pltpu.roll(inner, LEN - 1, 0))
        tap = [consts[4 + k : 5 + k, own_cols] for k in range(3)]
        conv = tap[0] * before + tap[1] * inner + tap[2] * after
        return (b * conv).astype(BF16)

    def spread(left, weight, part, reduce):
        rows = pl.ds(reduce.row, LEN)

        def block(y):
            piece = jnp.dot(left, weight[y], preferred_element_type=F32).astype(BF16)
            part[0, y, rows, :] = piece[:, :W]
            part[1, y, rows, :] = piece[:, W:]

        block(h.yo)
        reduce.start(h.yo, 0)
        others = (h.yp, h.ym, h.y)
        for y in others:
            block(y)
        for y in others:
            reduce.start(y, 1)

    def A(s, before_out=None):
        gated = mixer(s)
        if before_out:
            before_out()
        spread(gated, WO, PA, mix[s])

    def B(s):
        mix[s].b()

    def C(s):
        mix[s].c()

    def D(s):
        M[h.c, h.y, pl.ds(s * LEN, LEN), :] = mix[s].d().astype(BF16)
        mids[s].t0()

    def Ea(s):
        mids[s].t1()

    def Eb(s):
        mids[s].t1b()

    def F(s):
        mids[s].t2()

    def Ga(s):
        mids[s].t3()

        def tile(i, carry):
            rows = pl.ds(pl.multiple_of(s * LEN + i * TILE, TILE), TILE)
            mixed, kept = blocks(M, rows), blocks(X, rows)
            factor = mean_factor(total([ref[...].astype(F32) for ref in mixed]))
            for j in range(8):
                add = mixed[j][...].astype(F32) * factor * gain(1, j)
                kept[j][...] = (kept[j][...].astype(F32) + add).astype(BF16)
            scale_out(X, rows, 2)
            return carry

        lax.fori_loop(0, LEN // TILE, tile, 0)

    def Gb(s):
        rows = pl.ds(s * LEN, LEN)
        lifted = jnp.dot(N[rows, :], WU[...].reshape(8 * W, 4 * W), preferred_element_type=F32)
        lifted = jnp.maximum(lifted, 0.0)
        ACT[rows, :] = (lifted * lifted).astype(BF16)

    def H(s):
        spread(ACT[pl.ds(s * LEN, LEN), :], WD, PB, ffn[s])

    def D2(s):
        own = ffn[s].d()
        OWN[pl.ds(s * LEN, LEN), :] = own
        energy = jnp.sum((own * own).T, axis=0, keepdims=True)
        ST[s, h.col] = energy
        for dev in peers:
            stats.same(ST.at[s, h.col], known[s], dev)

    def finish(s):
        stats.landed(ST.at[s, pl.ds(0, 7)], known[s])
        factor = mean_factor(sum(ST[s, k] for k in range(8)))
        rows = pl.ds(s * LEN, LEN)
        wide = jnp.broadcast_to(factor, (128, LEN)).T
        wide = jnp.concatenate([wide, wide], axis=1)
        closing = OWN[rows, :] * wide * consts[3:4, own_cols]
        OUTV[rows, :] = (X[h.c, h.y, rows, :].astype(F32) + closing).astype(BF16)
        stored.append(pltpu.make_async_copy(OUTV.at[rows], out.at[rows], local.at[12 + s]))
        stored[-1].start()

    known, stored = link.arrivals(NSEQ), []

    loads[0].wait()
    toks[0].t0()
    toks[1].t0()
    for load in loads[1:4]:
        load.wait()
    bcv.p1(True)
    bcv.p1(False)
    loads[4].wait()
    outw.p1(True)
    outw.p1(False)
    for load in loads[5:]:
        load.wait()
    for k, g in enumerate((ga, gb, gc, gd)):
        consts[k : k + 1, :] = g[...].astype(F32)[None, :]
    consts[4:7, :] = taps[...].astype(F32)

    bcv.s1()
    bcv.own2()
    outw.s1()
    outw.own2()
    bcv.s2()
    outw.s2()
    toks[0].t1()
    toks[0].t1b()
    bcv.s3()
    toks[1].t1()
    toks[1].t1b()
    toks[0].t2()
    toks[0].t3()
    norm_tokens(0, 512)
    outw.s3()
    toks[1].t2()
    toks[1].t3()
    norm_tokens(512, 512)
    bcv.s4()
    up.p1(True)
    up.p1(False)
    up.own2()
    A(0, outw.s4)
    B(0)
    down.p1(True)
    down.p1(False)
    A(1)
    up.s1()
    B(1)
    C(0)
    down.own2()
    A(2)
    B(2)
    C(1)
    A(3)
    B(3)
    up.s2()
    D(0)
    C(2)
    down.s1()
    Ea(0)
    up.s3()
    D(1)
    C(3)
    Eb(0)
    F(0)
    down.s2()
    Ea(1)
    D(2)
    Eb(1)
    early.drain(X.at[:, :, pl.ds(0, 896)])
    Ga(0)
    F(1)
    D(3)
    Ea(2)
    up.s4()
    Gb(0)
    Eb(2)
    Ga(1)
    Ea(3)
    down.s3()
    Gb(1)
    Eb(3)
    F(2)
    F(3)
    Ga(2)
    Gb(2)
    Ga(3)
    Gb(3)
    down.s4()
    H(0)
    ffn[0].b()
    H(1)
    ffn[1].b()
    H(2)
    ffn[2].b()
    ffn[0].c()
    H(3)
    ffn[3].b()
    ffn[1].c()
    ffn[2].c()
    D2(0)
    ffn[3].c()
    D2(1)
    D2(2)
    finish(0)
    D2(3)
    finish(1)
    finish(2)
    finish(3)
    late.drain(M.at[:, :, pl.ds(0, 896)])
    sums.drain(PA.at[:, :, pl.ds(0, 896)])
    last.drain(PB.at[:, :, pl.ds(0, 896)])
    stats.drain(ST.at[:, pl.ds(0, 7)])
    for weight in (bcv, outw, up, down):
        weight.drain()
    for copy in stored:
        copy.wait()


def body(
    tokens, mix_in_gain, bgate_weight, cgate_weight, value_weight, conv_taps, out_weight,
    mix_out_gain, ffn_in_gain, up_weight, down_weight, ffn_out_gain,
):
    hbm = pl.BlockSpec(memory_space=pltpu.HBM)
    reduce_scratch = [
        pltpu.VMEM((2, 4, ROWS, W), BF16),
        pltpu.VMEM((4, ROWS, W), BF16),
        pltpu.VMEM((2, NSEQ, LEN // 2, W), BF16),
        pltpu.VMEM((2, ROWS, W), BF16),
    ]
    return pl.pallas_call(
        kernel,
        out_shape=jax.ShapeDtypeStruct((ROWS, W), BF16),
        in_specs=[hbm] * 12,
        out_specs=hbm,
        scratch_shapes=[
            pltpu.VMEM((8, 8 * W), F32),
            *[pltpu.VMEM((8 * W,), BF16)] * 4,
            pltpu.VMEM((3, 8 * W), BF16),
            pltpu.VMEM((2, 4, ROWS, W), BF16),
            pltpu.VMEM((2, 4, ROWS, W), BF16),
            pltpu.VMEM((ROWS, 8 * W), BF16),
            pltpu.VMEM((4, 512, 3 * W), BF16),
            pltpu.VMEM((4, W, 512), BF16),
            pltpu.VMEM((4, 512, 4 * W), BF16),
            pltpu.VMEM((4, 4 * W, 512), BF16),
            pltpu.VMEM((ROWS, 4 * W), BF16),
            *reduce_scratch,
            *reduce_scratch,
            pltpu.VMEM((ROWS, W), F32),
            pltpu.VMEM((NSEQ, 8, 1, W), F32),
            pltpu.VMEM((ROWS, W), BF16),
            pltpu.SemaphoreType.DMA((NSEND,)),
            pltpu.SemaphoreType.DMA((NRECV,)),
            pltpu.SemaphoreType.DMA((12 + NSEQ,)),
        ],
        compiler_params=pltpu.CompilerParams(
            collective_id=0, has_side_effects=True, vmem_limit_bytes=64 * 1024 * 1024 - 65536
        ),
    )(tokens, bgate_weight, cgate_weight, value_weight, out_weight, up_weight, down_weight,
      mix_in_gain, mix_out_gain, ffn_in_gain, ffn_out_gain, conv_taps)


def solution(mesh):
    torus = Mesh(mesh.devices.reshape(2, 4, 4, 4, 2), ("r", "z", "x", "y", "c"))
    fs, tp = ("z", "x"), ("y", "c")
    return jax.shard_map(
        body,
        mesh=torus,
        in_specs=(
            P(("r", "z", "x"), tp), P(), P(fs, tp), P(fs, tp), P(fs, tp), P(), P(tp, fs),
            P(), P(), P(fs, tp), P(tp, fs), P(),
        ),
        out_specs=P(("r", "z", "x"), tp),
        check_vma=False,
    )
```
